512 devices in a mesh: fs: 64 (over z, y), tp: 8 (over x, core).
Axes of the slice: x: 4, y: 8, z: 8, core: 2. Of those that a mesh axis runs over, the one named last changes fastest.
Arguments:
- tokens: bfloat16 [24576, 2048], P('fs', 'tp'), may hold values from -24 to 24, as said below
- mixer_gain: float32 [2048], replicated, may hold values from 0.1 to 1.9
- w_content: float32 [2048, 1024], P('fs', 'tp'), may hold values from -0.125 to 0.125
- w_spatial: float32 [2048, 1024], P('fs', 'tp'), may hold values from -0.125 to 0.125
- content_scale: float32 [1024], P('tp'), may hold values from 0.5 to 2
- spatial_scale: float32 [1024], P('tp'), may hold values from 0.2 to 3.5, as said below
- spatial_gain: float32 [1024], P('tp'), may hold values from 0.1 to 1.9
- block_mixing: bfloat16 [8, 128, 128], P('tp'), may hold values from -0.5 to 0.5
- block_bias: float32 [8, 128], P('tp'), may hold values from -6 to 6
- w_project: float32 [1024, 2048], P('tp', 'fs'), may hold values from -0.1875 to 0.1875
- project_scale: float32 [2048], P('fs'), may hold values from 0.5 to 2
- channel_gain: float32 [2048], replicated, may hold values from 0.1 to 1.9
- w_up: float32 [2048, 8192], P('fs', 'tp'), may hold values from -0.125 to 0.125
- up_scale: float32 [8192], P('tp'), may hold values from 0.5 to 2
- w_down: float32 [8192, 2048], P('tp', 'fs'), may hold values from -0.0625 to 0.0625
- down_scale: float32 [2048], P('fs'), may hold values from 0.5 to 2
Outputs:
- layer_out: bfloat16 [24576, 2048], P('fs', 'tp')
The draws below stay inside these ranges and needn't reach their ends.
Inputs may be any that keep to these rules, and one draw needn't show every extreme that they name: `tokens`: activations whose features and rows have differing scales. `spatial_scale`: positive column scales.
All inputs are finite; a program needn't handle non-finite values.
Results may differ from the reference program's by a relative error of at most 0.019.
Values may be sent and summed in bfloat16 or wider, within the bound.
A program may use at most 64 MiB of HBM per device.

```python
import math
import jax
import jax.numpy as jnp
from jax import lax

D = 2048
GROUPS = 8
GCH = 128
W_SGU = 1024
FF = 8192
BLOCK = 128
TOK_DEV = 384
TOKENS = 24576
N_FS = 64
N_TP = 8


def draw_tokens(key, part):
    first_key = jax.random.fold_in(key, 11)
    second_key = jax.random.fold_in(key, 12)
    third_key = jax.random.fold_in(key, 13)
    column_scales = jnp.exp(jax.random.uniform(second_key, (D,), jnp.float32, math.log(0.3), math.log(3.0)))
    base_values = jax.random.truncated_normal(first_key, -4.0, 4.0, (TOKENS, D), jnp.float32)
    row_scales = jnp.exp(jax.random.uniform(third_key, (TOKENS, 1), jnp.float32, math.log(0.5), math.log(2.0)))
    return (base_values * column_scales[None, :] * row_scales).astype(jnp.bfloat16)


def draw_spatial_scale(key, part):
    jitter_key = jax.random.fold_in(key, 21)
    position = jnp.arange(W_SGU).astype(jnp.float32) / (W_SGU - 1)
    jitter = jnp.exp(jax.random.uniform(jitter_key, (W_SGU,), jnp.float32, -0.35, 0.35))
    base_scale = jnp.exp(math.log(0.5) + (math.log(1.6) - math.log(0.5)) * position)
    return (base_scale * jitter).astype(jnp.float32)


def shard_levels(own_key, dims, shards, smallest, largest):
    factor_of = 1.0
    for dim, blocks in shards:
        heights = jax.random.uniform(jax.random.fold_in(jax.random.fold_in(own_key, 6), dim), (blocks,), jnp.float32, smallest / len(shards), largest / len(shards))
        factor_of = factor_of * jnp.repeat(jnp.exp(heights), dims[dim] // blocks).reshape((-1,) + (1,) * (len(dims) - 1 - dim))
    return factor_of


def scatter_about(stream_key, dims, scale, reach, split=(), kind=jnp.bfloat16):
    values = scale * jax.random.normal(stream_key, dims, jnp.float32)
    if split:
        values = values * shard_levels(stream_key, dims, split, -0.22, 0.18)
    return jnp.clip(values, -reach, reach).astype(kind)


def setup_inputs(seed: int = 0) -> dict:
    seeds = jax.random.split(jax.random.key(seed), 17)
    return {
        "tokens": draw_tokens(jax.random.fold_in(seeds[16], 71), 0),
        "mixer_gain": jnp.clip(1.0 + 0.18 * jax.random.normal(seeds[1], (D,), jnp.float32), 0.1, 1.9),
        "w_content": scatter_about(seeds[2], (D, W_SGU), D ** -0.5, 0.125, ((0, 64), (1, 8)), jnp.float32),
        "w_spatial": scatter_about(seeds[3], (D, W_SGU), D ** -0.5, 0.125, ((0, 64), (1, 8)), jnp.float32),
        "content_scale": jnp.clip(jnp.exp(math.log(2.0) - 1.3862944 * jax.random.uniform(seeds[4], (W_SGU,), jnp.float32) ** shard_levels(seeds[4], (W_SGU,), ((0, 8),), -0.2, 0.2)), 0.5, 2.0),
        "spatial_scale": draw_spatial_scale(jax.random.fold_in(seeds[16], 71), 0),
        "spatial_gain": jnp.clip(1.0 + 0.18 * jax.random.normal(seeds[6], (W_SGU,), jnp.float32), 0.1, 1.9),
        "block_mixing": scatter_about(seeds[7], (GROUPS, BLOCK, BLOCK), BLOCK ** -0.5, 0.5, ((0, 8),)),
        "block_bias": scatter_about(seeds[8], (GROUPS, BLOCK), 1.0, 6.0, ((0, 8),), jnp.float32),
        "w_project": scatter_about(seeds[9], (W_SGU, D), W_SGU ** -0.5, 0.1875, ((0, 8), (1, 64)), jnp.float32),
        "project_scale": jnp.clip(jnp.exp(math.log(2.0) - 1.3862944 * jax.random.uniform(seeds[10], (D,), jnp.float32) ** shard_levels(seeds[10], (D,), ((0, 64),), -0.2, 0.2)), 0.5, 2.0),
        "channel_gain": jnp.clip(1.0 + 0.18 * jax.random.normal(seeds[11], (D,), jnp.float32), 0.1, 1.9),
        "w_up": scatter_about(seeds[12], (D, FF), D ** -0.5, 0.125, ((0, 64), (1, 8)), jnp.float32),
        "up_scale": jnp.clip(jnp.exp(math.log(2.0) - 1.3862944 * jax.random.uniform(seeds[13], (FF,), jnp.float32) ** shard_levels(seeds[13], (FF,), ((0, 8),), -0.2, 0.2)), 0.5, 2.0),
        "w_down": scatter_about(seeds[14], (FF, D), FF ** -0.5, 0.0625, ((0, 8), (1, 64)), jnp.float32),
        "down_scale": jnp.clip(jnp.exp(math.log(2.0) - 1.3862944 * jax.random.uniform(seeds[15], (D,), jnp.float32) ** shard_levels(seeds[15], (D,), ((0, 64),), -0.2, 0.2)), 0.5, 2.0),
    }


EPSILON = 1e-06

def normalize_rows(token_rows, gain_vector):
    values = token_rows.astype(jnp.float32)
    scaled = values * lax.rsqrt(lax.optimization_barrier(jnp.mean(values * values, axis=-1, keepdims=True)) + EPSILON)
    return (scaled * gain_vector).astype(jnp.bfloat16)

def split_sum(left, right, column_scale, shard_count):
    shard_width = left.shape[1] // shard_count
    running = jnp.zeros((left.shape[0], right.shape[1]), jnp.float32)
    for shard_index in range(shard_count):
        low = shard_index * shard_width
        partial_value = jnp.dot(left[:, low:low + shard_width], right[low:low + shard_width, :], preferred_element_type=jnp.float32) * column_scale
        rounded = lax.optimization_barrier(partial_value.astype(jnp.bfloat16))
        running = running + rounded.astype(jnp.float32)
    return running

def reference(tokens, mixer_gain, w_content, w_spatial, content_scale, spatial_scale, spatial_gain, block_mixing, block_bias, w_project, project_scale, channel_gain, w_up, up_scale, w_down, down_scale):
    content_weight = w_content.astype(jnp.bfloat16)
    spatial_weight = w_spatial.astype(jnp.bfloat16)
    project_weight = w_project.astype(jnp.bfloat16)
    up_weight = w_up.astype(jnp.bfloat16)
    down_weight = w_down.astype(jnp.bfloat16)
    causal_mask = jnp.tril(jnp.ones((BLOCK, BLOCK), dtype=bool))
    mixing_weights = jnp.where(causal_mask[None, :, :], block_mixing.astype(jnp.float32), jnp.float32(0.0))

    def one_sequence(token_rows):
        normed = normalize_rows(token_rows, mixer_gain)
        content = jax.nn.gelu(jnp.dot(normed, content_weight, preferred_element_type=jnp.float32) * content_scale)
        spatial = jax.nn.gelu(jnp.dot(normed, spatial_weight, preferred_element_type=jnp.float32) * spatial_scale)
        spatial_norm = (spatial * lax.rsqrt(lax.optimization_barrier(jnp.mean(spatial * spatial, axis=-1, keepdims=True)) + EPSILON) * spatial_gain).astype(jnp.bfloat16)
        grouped = spatial_norm.astype(jnp.float32).reshape(TOK_DEV // BLOCK, BLOCK, GROUPS, GCH)
        mixed_block = jnp.einsum('gts,nsgc->ntgc', mixing_weights, grouped) + block_bias.T[None, :, :, None]
        gated = (content * mixed_block.reshape(TOK_DEV, W_SGU)).astype(jnp.bfloat16)
        mixer_sum = split_sum(gated, project_weight, project_scale, N_TP)
        middle = (token_rows.astype(jnp.float32) + mixer_sum).astype(jnp.bfloat16)
        channel_normed = normalize_rows(middle, channel_gain)
        up_linear = jnp.dot(channel_normed, up_weight, preferred_element_type=jnp.float32) * up_scale
        hidden = jnp.square(jax.nn.relu(up_linear)).astype(jnp.bfloat16)
        channel_sum = split_sum(hidden, down_weight, down_scale, N_TP)
        return (middle.astype(jnp.float32) + channel_sum).astype(jnp.bfloat16)
    layer_out = lax.map(one_sequence, tokens.reshape(N_FS, TOK_DEV, D))
    return layer_out.reshape(TOKENS, D)
```

```python
import jax
import jax.numpy as jnp
from jax import lax
from jax.experimental import pallas as pl
from jax.experimental.pallas import tpu as pltpu
from jax.sharding import PartitionSpec as P

EPSILON = 1e-06
MESH = pl.DeviceIdType.MESH
F32 = jnp.float32
BF16 = jnp.bfloat16

RING = 8
HOPS = RING // 2
CHIPS_X = 4
N_TP = 2 * CHIPS_X
SLICE = 32
BLOCK = 128
WIDTHS = (384, 256, 256, 512, 512, 512)


def nt_dot(left, right):
    return lax.dot_general(left, right, (((1,), (1,)), ((), ())), preferred_element_type=F32)


def layer_kernel(
    tokens_ref, mixer_gain_ref, w_content_ref, w_spatial_ref, content_scale_ref, spatial_scale_ref,
    spatial_gain_ref, mixing_ref, bias_ref, w_project_ref, project_scale_ref, channel_gain_ref,
    w_up_ref, up_scale_ref, w_down_ref, down_scale_ref,
    out_ref,
    w0, w1, w2, w3, w4, w5, tok1, tok2, normed, squares, hidden, acc,
    sib_out, sib_in, ring_out, far_in, near_in,
    w_send, w_recv, ag_send, ag_recv, rs_send, rs_recv, sq_send, sq_recv,
):
    chunks = (w0, w1, w2, w3, w4, w5)
    fs, tp = lax.axis_index("fs"), lax.axis_index("tp")
    z, y = fs // RING, fs % RING
    x, core = tp // 2, tp % 2
    p = jnp.where(core == 0, y, z)
    q = jnp.where(core == 0, z, y)

    def fs_of(pp, qq):
        return jnp.where(core == 0, qq * RING + pp, pp * RING + qq)

    def tp_of(dx, other):
        c = (1 - core) if other else core
        return 2 * ((x + dx + CHIPS_X) % CHIPS_X) + c

    first_next = (fs_of((p + 1) % RING, q), fs_of((p + RING - 1) % RING, q))
    second_next = (fs_of(p, (q + 1) % RING), fs_of(p, (q + RING - 1) % RING))

    def remote(src, dst, ss, rs, to_fs, to_tp):
        return pltpu.make_async_remote_copy(
            src_ref=src, dst_ref=dst, send_sem=ss, recv_sem=rs,
            device_id=(to_fs, to_tp), device_id_type=MESH,
        )

    eye = (
        lax.broadcasted_iota(jnp.int32, (SLICE, SLICE), 0)
        == lax.broadcasted_iota(jnp.int32, (SLICE, SLICE), 1)
    ).astype(F32).astype(BF16)

    def turned(w, scale):
        scaled = (w.astype(BF16).astype(F32) * scale).astype(BF16)
        return nt_dot(eye, scaled).astype(BF16)

    w0[q, p, :, 0:128] = w_content_ref[...].astype(BF16)
    w0[q, p, :, 128:256] = w_spatial_ref[...].astype(BF16)
    w0[q, p, :, 256:384] = turned(w_project_ref[...], project_scale_ref[...])
    w1[q, p] = w_up_ref[:, 0:256].astype(BF16)
    w2[q, p] = w_up_ref[:, 256:512].astype(BF16)
    w3[q, p] = w_up_ref[:, 512:1024].astype(BF16)
    w4[q, p] = turned(w_down_ref[0:512], down_scale_ref[...])
    w5[q, p] = turned(w_down_ref[512:1024], down_scale_ref[...])
    tok1[tp] = tokens_ref[...]

    barrier = pltpu.get_barrier_semaphore()
    for to in first_next + second_next:
        pl.semaphore_signal(barrier, inc=1, device_id=(to, tp), device_id_type=MESH)
    for d in range(1, N_TP):
        pl.semaphore_signal(barrier, inc=1, device_id=(fs, (tp + d) % N_TP), device_id_type=MESH)
    pl.semaphore_wait(barrier, 4 + N_TP - 1)

    def weight_copy(ci, phase, way, step, arriving=False):
        shift = step + (1 if arriving else 0)
        if way == 0:
            shift = -shift
        sems = (w_send.at[ci, phase, way, step], w_recv.at[ci, phase, way, step])
        if phase == 0:
            ref = chunks[ci].at[q, (p + shift + RING) % RING]
            if step == HOPS - 1:
                ref = ref.at[pl.ds(way * (SLICE // 2), SLICE // 2)]
            return remote(ref, ref, *sems, first_next[way], tp)
        ref = chunks[ci].at[(q + shift + RING) % RING]
        if step == HOPS - 1:
            ref = ref.at[pl.ds(way * (RING // 2), RING // 2)]
        return remote(ref, ref, *sems, second_next[way], tp)

    def send(ci, phase, step):
        for way in range(2):
            weight_copy(ci, phase, way, step).start()

    def arrived(ci, phase, step):
        for way in range(2):
            weight_copy(ci, phase, way, step, arriving=True).wait_recv()

    def forward(ci, phase, step):
        for way in range(2):
            weight_copy(ci, phase, way, step - 1, arriving=True).wait_recv()
            weight_copy(ci, phase, way, step).start()

    def second_start(ci):
        arrived(ci, 0, HOPS - 1)
        send(ci, 1, 0)

    half = tokens_ref.shape[0] // 2

    class Gather:
        def __init__(self, buf, n):
            self.buf, self.n = buf, n

        def copy(self, k, arriving=False):
            dx = (0, -1, 1, 2, 0, 0, -1, 1)[k]
            if arriving and k >= 4:
                dx = (-1, 1, -2, 2)[k - 4]
            ref = self.buf.at[tp_of(dx, arriving and k < 4)]
            if k >= 6:
                ref = ref.at[pl.ds((k - 6) * half, half)]
            to = tp_of(0, True) if k < 4 else tp_of((1, -1)[k % 2], False)
            return remote(ref, ref, ag_send.at[self.n, k], ag_recv.at[self.n, k], fs, to)

        def begin(self):
            for k in (4, 5, 0):
                self.copy(k).start()

        def pass_on(self):
            for k in range(2):
                self.copy(4 + k, True).wait_recv()
                self.copy(6 + k).start()
                self.copy(1 + k).start()

        def far(self):
            for k in range(2):
                self.copy(6 + k, True).wait_recv()
            self.copy(3).start()

        def finish(self):
            for k in range(4):
                self.copy(k, True).wait_recv()

        def drain(self):
            for k in range(8):
                self.copy(k).wait_send()

    class Scatter:
        order = (2, 1, -1, 0)

        def __init__(self, n):
            self.n = n

        def sems(self, k):
            return rs_send.at[self.n, k], rs_recv.at[self.n, k]

        def across(self, k):
            return remote(sib_out.at[self.n, k], sib_in.at[self.n, k], *self.sems(k), fs, tp_of(0, True))

        def far(self, way):
            rows = pl.ds(way * half, half)
            return remote(ring_out.at[self.n, 0, rows], far_in.at[self.n, way], *self.sems(4 + way),
                          fs, tp_of((1, -1)[way], False))

        def near(self, way, part):
            rows = pl.ds(part * half, half)
            return remote(ring_out.at[self.n, 1 + way, rows], near_in.at[self.n, way, rows],
                          *self.sems(6 + 2 * way + part), fs, tp_of((1, -1)[way], False))

        def begin(self, block_of):
            for k, dx in enumerate(self.order):
                sib_out[self.n, k] = block_of(k, dx, True).astype(BF16)
                self.across(k).start()
                if k > 0:
                    self.own(block_of, k - 1)
            self.own(block_of, 3)

        def own(self, block_of, k):
            n = self.n
            value = block_of(k, self.order[k], False)
            self.across(k).wait_recv()
            value = value + sib_in[n, k].astype(F32)
            if k == 0:
                ring_out[n, 0] = value.astype(BF16)
                self.far(0).start()
                self.far(1).start()
            else:
                acc[k - 1] = value
                if k < 3:
                    way = k - 1
                    part = 1 - way
                    ring_out[n, k, part * half:(part + 1) * half] = (
                        value[part * half:(part + 1) * half].astype(BF16))
                    self.near(way, part).start()

        def combine(self):
            n = self.n
            for way in range(2):
                self.far(way).wait_recv()
                rows = slice(way * half, (way + 1) * half)
                ring_out[n, 1 + way, rows] = (acc[way, rows] + far_in[n, way].astype(F32)).astype(BF16)
                self.near(way, way).start()

        def finish(self):
            for way in range(2):
                for part in range(2):
                    self.near(way, part).wait_recv()
            n = self.n
            return acc[2] + near_in[n, 0].astype(F32) + near_in[n, 1].astype(F32)

        def drain(self):
            for k in range(4):
                self.across(k).wait_send()
            for way in range(2):
                self.far(way).wait_send()
                for part in range(2):
                    self.near(way, part).wait_send()

    width = tokens_ref.shape[1]

    def normalize(buf, gain_ref):
        total = None
        for t in range(N_TP):
            v = buf[t].astype(F32)
            s = jnp.sum(v * v, axis=1, keepdims=True)
            total = s if total is None else total + s
        r = lax.rsqrt(total / (N_TP * width) + EPSILON)
        for t in range(N_TP):
            cols = slice(t * width, (t + 1) * width)
            normed[:, cols] = (buf[t].astype(F32) * r * gain_ref[:, cols]).astype(BF16)

    def weight_rows(ref, zz, cols):
        pieces = []
        for j in range(RING):
            pieces.append(ref[jnp.where(core == 0, zz, j), jnp.where(core == 0, j, zz), :, cols])
        return jnp.concatenate(pieces, axis=0)

    def all_rows(ref, cols):
        return jnp.concatenate([weight_rows(ref, zz, cols) for zz in range(RING)], axis=0)

    gather1, gather2 = Gather(tok1, 0), Gather(tok2, 1)
    scatter1, scatter2 = Scatter(0), Scatter(1)
    every = range(len(chunks))

    send(0, 0, 0)
    gather1.begin()
    for ci in every[1:]:
        send(ci, 0, 0)
    for step in range(1, HOPS):
        for ci in every:
            forward(ci, 0, step)
        if step == HOPS - 2:
            gather1.pass_on()
    second_start(0)
    second_start(1)
    gather1.far()
    gather1.finish()
    normalize(tok1, mixer_gain_ref)
    forward(0, 1, 1)
    forward(1, 1, 1)
    second_start(2)
    forward(0, 1, 2)
    forward(1, 1, 2)
    second_start(3)
    forward(0, 1, 3)
    forward(1, 1, 3)
    arrived(0, 1, 3)

    linear = jnp.dot(normed[...], all_rows(w0, slice(0, 256)), preferred_element_type=F32)
    spatial = jax.nn.gelu(linear[:, 128:256] * spatial_scale_ref[...])
    sq = spatial * spatial
    sq_high = sq.astype(BF16)
    sq_low = (sq - sq_high.astype(F32)).astype(BF16)
    ones = jnp.ones((8, 128), BF16)
    squares[tp] = nt_dot(ones, sq_high) + nt_dot(ones, sq_low)

    def square_copy(d, arriving=False):
        ref = squares.at[(tp + N_TP - d) % N_TP] if arriving else squares.at[tp]
        return remote(ref, ref, sq_send.at[d - 1], sq_recv.at[d - 1], fs, (tp + d) % N_TP)

    for d in range(1, N_TP):
        square_copy(d).start()
    content = jax.nn.gelu(linear[:, 0:128] * content_scale_ref[...])
    gained = (spatial * spatial_gain_ref[...]).astype(BF16)
    causal = (
        lax.broadcasted_iota(jnp.int32, (BLOCK, BLOCK), 1)
        <= lax.broadcasted_iota(jnp.int32, (BLOCK, BLOCK), 0)
    )
    mixing = jnp.where(causal, mixing_ref[0].astype(F32), 0.0)
    bias = jnp.transpose(jnp.broadcast_to(bias_ref[...], (BLOCK, BLOCK)))
    forward(2, 1, 1)
    forward(3, 1, 1)
    arrived(1, 1, 3)
    for d in range(1, N_TP):
        square_copy(d, True).wait_recv()
    total_sq = squares[0]
    for t in range(1, N_TP):
        total_sq = total_sq + squares[t]
    row_scale = lax.rsqrt(total_sq[0:1] / (N_TP * 128) + EPSILON)
    gated_blocks = []
    for b in range(tokens_ref.shape[0] // BLOCK):
        rows = slice(b * BLOCK, (b + 1) * BLOCK)
        scaled = (mixing * row_scale[:, rows]).astype(BF16)
        mixed = jnp.dot(scaled, gained[rows], preferred_element_type=F32) + bias
        gated_blocks.append((content[rows] * mixed).astype(BF16))
    gated = jnp.concatenate(gated_blocks, axis=0)

    def project_block(k, dx, other):
        return nt_dot(gated, weight_rows(w0, tp_of(dx, other), slice(256, 384)))

    scatter1.begin(project_block)
    forward(2, 1, 2)
    forward(3, 1, 2)
    second_start(4)
    scatter1.combine()
    forward(2, 1, 3)
    forward(3, 1, 3)
    second_start(5)
    middle = tokens_ref[...].astype(F32) + scatter1.finish()
    tok2[tp] = middle.astype(BF16)
    gather2.begin()
    arrived(2, 1, 3)
    arrived(3, 1, 3)
    gather2.pass_on()
    forward(4, 1, 1)
    gather2.far()
    gather2.finish()
    forward(5, 1, 1)
    normalize(tok2, channel_gain_ref)

    at = 0
    for ref in (w1, w2, w3):
        for low in range(0, ref.shape[3], 256):
            up = jnp.dot(normed[...], all_rows(ref, slice(low, low + 256)), preferred_element_type=F32)
            up = jnp.maximum(up * up_scale_ref[:, at:at + 256], 0.0)
            hidden[:, at:at + 256] = (up * up).astype(BF16)
            at += 256
    forward(4, 1, 2)
    forward(5, 1, 2)
    forward(4, 1, 3)
    forward(5, 1, 3)
    arrived(4, 1, 3)

    slots = [(k, other) for k in range(4) for other in (True, False)]
    for i, (k, other) in enumerate(slots):
        zz = tp_of(Scatter.order[k], other)
        acc[3 + i] = nt_dot(hidden[:, 0:512], weight_rows(w4, zz, slice(0, 512)))
    arrived(5, 1, 3)

    def down_block(k, dx, other):
        return acc[3 + 2 * k + (0 if other else 1)] + nt_dot(
            hidden[:, 512:1024], weight_rows(w5, tp_of(dx, other), slice(0, 512)))

    scatter2.begin(down_block)
    scatter2.combine()
    out_ref[...] = (tok2[tp].astype(F32) + scatter2.finish()).astype(BF16)

    for ci in every:
        for phase in range(2):
            for way in range(2):
                for step in range(HOPS):
                    weight_copy(ci, phase, way, step).wait_send()
    gather1.drain()
    gather2.drain()
    scatter1.drain()
    scatter2.drain()
    for d in range(1, N_TP):
        square_copy(d).wait_send()


def shards(
    tokens, mixer_gain, w_content, w_spatial, content_scale, spatial_scale, spatial_gain, block_mixing,
    block_bias, w_project, project_scale, channel_gain, w_up, up_scale, w_down, down_scale,
):
    rows, width = tokens.shape
    row = lambda v: v.reshape(1, -1)
    chunk = lambda n: pltpu.VMEM((RING, RING, SLICE, n), BF16)
    vmem = pl.BlockSpec(memory_space=pltpu.VMEM)
    dma = pltpu.SemaphoreType.DMA
    return pl.pallas_call(
        layer_kernel,
        out_shape=jax.ShapeDtypeStruct((rows, width), BF16),
        in_specs=[vmem] * 16,
        out_specs=vmem,
        scratch_shapes=[chunk(n) for n in WIDTHS] + [
            pltpu.VMEM((N_TP, rows, width), BF16),
            pltpu.VMEM((N_TP, rows, width), BF16),
            pltpu.VMEM((rows, N_TP * width), BF16),
            pltpu.VMEM((N_TP, 8, rows), F32),
            pltpu.VMEM((rows, w_up.shape[1]), BF16),
            pltpu.VMEM((11, rows, width), F32),
            pltpu.VMEM((2, 4, rows, width), BF16),
            pltpu.VMEM((2, 4, rows, width), BF16),
            pltpu.VMEM((2, 3, rows, width), BF16),
            pltpu.VMEM((2, 2, rows // 2, width), BF16),
            pltpu.VMEM((2, 2, rows, width), BF16),
            dma((len(WIDTHS), 2, 2, HOPS)), dma((len(WIDTHS), 2, 2, HOPS)),
            dma((2, 8)), dma((2, 8)), dma((2, 10)), dma((2, 10)), dma((7,)), dma((7,)),
        ],
        compiler_params=pltpu.CompilerParams(
            collective_id=0, has_side_effects=True, vmem_limit_bytes=56 * 1024 * 1024),
        name="layer",
    )(
        tokens, row(mixer_gain), w_content, w_spatial, row(content_scale), row(spatial_scale),
        row(spatial_gain), block_mixing, block_bias, w_project, row(project_scale), row(channel_gain),
        w_up, row(up_scale), w_down, row(down_scale),
    )


def solution(mesh):
    return jax.shard_map(
        shards,
        mesh=mesh,
        in_specs=(
            P("fs", "tp"), P(), P("fs", "tp"), P("fs", "tp"), P("tp"), P("tp"), P("tp"),
            P("tp", None, None), P("tp", None), P("tp", "fs"), P("fs"), P(), P("fs", "tp"), P("tp"),
            P("tp", "fs"), P("fs"),
        ),
        out_specs=P("fs", "tp"),
        check_vma=False,
    )
```

```python
import jax
import jax.numpy as jnp
from jax import lax
from jax.experimental import pallas as pl
from jax.experimental.pallas import tpu as pltpu
from jax.sharding import PartitionSpec as P

EPSILON = 1e-06
MESH = pl.DeviceIdType.MESH
F32 = jnp.float32
BF16 = jnp.bfloat16

RING = 8
HOPS = RING // 2
CHIPS_X = 4
N_TP = 2 * CHIPS_X
SLICE = 32
BLOCK = 128
N_INPUTS = 16


def nt_dot(left, right):
    return lax.dot_general(left, right, (((1,), (1,)), ((), ())), preferred_element_type=F32)


def layer_kernel(*refs):
    hbm = refs[:N_INPUTS]
    out_hbm = refs[N_INPUTS]
    inputs = refs[N_INPUTS + 1:2 * N_INPUTS + 1]
    (
        tokens_ref, mixer_gain_ref, w_content_ref, w_spatial_ref, content_scale_ref, spatial_scale_ref,
        spatial_gain_ref, mixing_ref, bias_ref, w_project_ref, project_scale_ref, channel_gain_ref,
        w_up_ref, up_scale_ref, w_down_ref, down_scale_ref,
    ) = inputs
    (
        wa, wb, wu, wd0, wd1, tok1, tok2, normed, squares, hidden, partial, out_ref,
        sib_out1, sib_in1, ring_out1, far_in1, near_in1, acc1,
        sib_out2, sib_in2, ring_out2, far_in2, near_in2, acc2,
        in_sem, out_sem, w1_send, w1_recv, w2_send, w2_recv,
        ag_send, ag_recv, rs_send, rs_recv, sq_send, sq_recv,
    ) = refs[2 * N_INPUTS + 1:]
    fs, tp = lax.axis_index("fs"), lax.axis_index("tp")
    z, y = fs // RING, fs % RING
    x, core = tp // 2, tp % 2
    p = jnp.where(core == 0, y, z)
    q = jnp.where(core == 0, z, y)

    def fs_of(pp, qq):
        return jnp.where(core == 0, qq * RING + pp, pp * RING + qq)

    def tp_of(dx, other):
        c = (1 - core) if other else core
        return 2 * ((x + dx + CHIPS_X) % CHIPS_X) + c

    first_next = (fs_of((p + 1) % RING, q), fs_of((p + RING - 1) % RING, q))
    second_next = (fs_of(p, (q + 1) % RING), fs_of(p, (q + RING - 1) % RING))

    barrier = pltpu.get_barrier_semaphore()
    for to in first_next + second_next:
        pl.semaphore_signal(barrier, inc=1, device_id=(to, tp), device_id_type=MESH)
    for d in range(1, N_TP):
        pl.semaphore_signal(barrier, inc=1, device_id=(fs, (tp + d) % N_TP), device_id_type=MESH)
    fetches = [pltpu.make_async_copy(hbm[i], inputs[i], in_sem.at[i]) for i in range(N_INPUTS)]
    for i in (2, 3, 9, 10, 0, 12, 14, 15, 1, 4, 5, 6, 7, 8, 11, 13):
        fetches[i].start()

    def remote(src, dst, ss, rs, to_fs, to_tp):
        return pltpu.make_async_remote_copy(
            src_ref=src, dst_ref=dst, send_sem=ss, recv_sem=rs,
            device_id=(to_fs, to_tp), device_id_type=MESH,
        )

    eye = (
        lax.broadcasted_iota(jnp.int32, (SLICE, SLICE), 0)
        == lax.broadcasted_iota(jnp.int32, (SLICE, SLICE), 1)
    )

    def scaled(w, scale):
        column = jnp.sum(jnp.where(eye, scale, 0.0), axis=1, keepdims=True)
        return (w.astype(BF16).astype(F32) * column).astype(BF16)

    for i in (2, 3, 9, 10):
        fetches[i].wait()
    wa[q, p, :, 0:128] = w_content_ref[...].astype(BF16)
    wa[q, p, :, 128:256] = w_spatial_ref[...].astype(BF16)
    wb[q, p] = scaled(w_project_ref[...], project_scale_ref[...])
    for i in (0, 12, 14, 15):
        fetches[i].wait()
    tok1[tp] = tokens_ref[...]
    down = scaled(w_down_ref[...], down_scale_ref[...])
    for k in range(2):
        cols = slice(k * 512, (k + 1) * 512)
        wu[k, q, p] = w_up_ref[:, cols].astype(BF16)
        wd0[k, q, p] = down[0:16, cols]
        wd1[k, q, p] = down[16:32, cols]
    pl.semaphore_wait(barrier, 4 + N_TP - 1)

    A, B, U, D0, D1 = range(5)
    first_units = (wa, wb, wu, wd0, wd1)

    def first_copy(u, way, step):
        at = (p + (step if way else -step) + RING) % RING
        if u in (A, B):
            ref = first_units[u].at[q, at]
            if step == HOPS - 1:
                ref = ref.at[pl.ds(way * (SLICE // 2), SLICE // 2)]
        elif step == HOPS - 1:
            ref = first_units[u].at[way, q, at]
        else:
            ref = first_units[u].at[:, q, at]
        return remote(ref, ref, w1_send.at[u], w1_recv.at[u, step], first_next[way], tp)

    def first_send(u, step):
        for way in range(2):
            first_copy(u, way, step).start()

    def first_wait(u, step):
        ref = first_units[u].at[0, 0] if u in (A, B) else first_units[u].at[:, 0, 0]
        if step < HOPS - 1:
            ref = first_units[u].at[0, 0:2] if u in (A, B) else first_units[u].at[:, 0, 0:2]
        remote(ref, ref, w1_send.at[u], w1_recv.at[u, step], first_next[0], tp).wait_recv()

    def first_forward(u, step):
        first_wait(u, step - 1)
        first_send(u, step)

    U0, U1, E0, E1, E2 = 2, 3, 4, 5, 6
    second_units = (wa, wb, wu.at[0], wu.at[1], wd0, wd1.at[0], wd1.at[1])

    def second_copy(u, way, step):
        at = (q + (step if way else -step) + RING) % RING
        ref = second_units[u].at[:, at] if u == E0 else second_units[u].at[at]
        if step == HOPS - 1:
            rows = pl.ds(way * HOPS, HOPS)
            ref = ref.at[:, rows] if u == E0 else ref.at[rows]
        return remote(ref, ref, w2_send.at[u], w2_recv.at[u, step], second_next[way], tp)

    def second_send(u, step=0):
        for way in range(2):
            second_copy(u, way, step).start()

    def second_wait(u, step=HOPS - 1):
        n = 1 if step == HOPS - 1 else 2
        ref = second_units[u].at[:, 0:n] if u == E0 else second_units[u].at[0:n]
        remote(ref, ref, w2_send.at[u], w2_recv.at[u, step], second_next[0], tp).wait_recv()

    def forward(u, step):
        second_wait(u, step - 1)
        second_send(u, step)

    half = tokens_ref.shape[0] // 2

    class Gather:
        def __init__(self, buf, n):
            self.buf, self.n = buf, n

        def copy(self, k, arriving=False):
            dx = (0, -1, 1, 2, 0, 0, -1, 1)[k]
            if arriving and k >= 4:
                dx = (-1, 1, -2, 2)[k - 4]
            ref = self.buf.at[tp_of(dx, arriving and k < 4)]
            if k >= 6:
                ref = ref.at[pl.ds((k - 6) * half, half)]
            to = tp_of(0, True) if k < 4 else tp_of((1, -1)[k % 2], False)
            return remote(ref, ref, ag_send.at[self.n], ag_recv.at[self.n, k], fs, to)

        def begin(self):
            for k in (4, 5, 0):
                self.copy(k).start()

        def pass_on(self):
            for k in range(2):
                self.copy(4 + k, True).wait_recv()
                self.copy(6 + k).start()
                self.copy(1 + k).start()

        def far(self):
            for k in range(2):
                self.copy(6 + k, True).wait_recv()
            self.copy(3).start()

        def finish(self):
            for k in range(4):
                self.copy(k, True).wait_recv()

        def drain(self):
            ref = self.buf.at[0:7]
            remote(ref, ref, ag_send.at[self.n], ag_recv.at[self.n, 0], fs, tp_of(1, False)).wait_send()

    class Scatter:
        order = (2, 1, -1, 0)

        def __init__(self, n, bufs, bytes_ref):
            self.n, self.bytes_ref = n, bytes_ref
            self.sib_out, self.sib_in, self.ring_out, self.far_in, self.near_in, self.acc = bufs

        def copy(self, src, dst, k, to):
            return remote(src, dst, rs_send.at[self.n], rs_recv.at[self.n, k], fs, to)

        def across(self, k):
            return self.copy(self.sib_out.at[k], self.sib_in.at[k], k, tp_of(0, True))

        def far(self, way):
            return self.copy(self.ring_out.at[0, pl.ds(way * half, half)], self.far_in.at[way], 4 + way,
                             tp_of((1, -1)[way], False))

        def near(self, way, part):
            rows = pl.ds(part * half, half)
            return self.copy(self.ring_out.at[1 + way, rows], self.near_in.at[way, rows], 6 + 2 * way + part,
                             tp_of((1, -1)[way], False))

        def begin(self, blocks_of):
            for k, dx in enumerate(self.order):
                across, own = blocks_of(k, dx)
                self.sib_out[k] = across.astype(BF16)
                self.across(k).start()
                self.acc[k] = own
                if k > 0:
                    self.own(k - 1)
            self.own(3)

        def own(self, k):
            self.across(k).wait_recv()
            value = self.acc[k] + self.sib_in[k].astype(F32)
            if k == 0:
                self.ring_out[0] = value.astype(BF16)
                self.far(0).start()
                self.far(1).start()
            else:
                self.acc[k] = value
                if k < 3:
                    part = 2 - k
                    rows = slice(part * half, (part + 1) * half)
                    self.ring_out[k, rows] = value[rows].astype(BF16)
                    self.near(k - 1, part).start()

        def combine(self):
            for way in range(2):
                self.far(way).wait_recv()
                rows = slice(way * half, (way + 1) * half)
                self.ring_out[1 + way, rows] = (
                    self.acc[1 + way, rows] + self.far_in[way].astype(F32)).astype(BF16)
                self.near(way, way).start()

        def finish(self):
            for way in range(2):
                for part in range(2):
                    self.near(way, part).wait_recv()
            return self.acc[3] + self.near_in[0].astype(F32) + self.near_in[1].astype(F32)

        def drain(self):
            remote(self.bytes_ref, self.bytes_ref, rs_send.at[self.n], rs_recv.at[self.n, 0], fs,
                   tp_of(1, False)).wait_send()

    width = tokens_ref.shape[1]

    def normalize(buf, gain_ref):
        total = None
        for t in range(N_TP):
            v = buf[t].astype(F32)
            s = jnp.sum(v * v, axis=1, keepdims=True)
            total = s if total is None else total + s
        r = lax.rsqrt(total / (N_TP * width) + EPSILON)
        for t in range(N_TP):
            cols = slice(t * width, (t + 1) * width)
            normed[:, cols] = (buf[t].astype(F32) * r * gain_ref[:, cols]).astype(BF16)

    def plane_rows(ref, zz, cols):
        return [ref[jnp.where(core == 0, zz, j), jnp.where(core == 0, j, zz), :, cols] for j in range(RING)]

    def all_rows(ref, cols):
        return jnp.concatenate([r for zz in range(RING) for r in plane_rows(ref, zz, cols)], axis=0)

    def set_of(*bufs, low=None):
        return bufs if low is None else tuple(b.at[pl.ds(low * (b.shape[0] // 2), b.shape[0] // 2)] for b in bufs)

    gather1, gather2 = Gather(tok1, 0), Gather(tok2, 1)
    bufs2 = (sib_out2, sib_in2, ring_out2, far_in2, near_in2, acc2)
    scatter1 = Scatter(0, (sib_out1, sib_in1, ring_out1, far_in1, near_in1, acc1), tok1.at[0:7])
    scatter2 = Scatter(1, set_of(*bufs2, low=0), sib_out2.at[0:7])
    scatter3 = Scatter(2, set_of(*bufs2, low=1), sib_out2.at[0:7])

    first_send(A, 0)
    first_send(B, 0)
    gather1.begin()
    first_send(U, 0)
    first_send(D0, 0)
    first_send(D1, 0)
    first_forward(A, 1)
    first_forward(B, 1)
    first_forward(U, 1)
    first_forward(D0, 1)
    first_forward(D1, 1)
    first_forward(A, 2)
    first_forward(B, 2)
    first_forward(U, 2)
    first_forward(D0, 2)
    first_forward(D1, 2)
    first_forward(A, 3)
    first_forward(B, 3)
    gather1.pass_on()
    first_forward(U, 3)
    first_forward(D0, 3)
    first_forward(D1, 3)
    first_wait(A, 3)
    second_send(A)
    first_wait(B, 3)
    second_send(B)
    for i in (1, 4, 5, 6, 7, 8, 11, 13):
        fetches[i].wait()
    gather1.far()
    first_wait(D1, 3)
    second_send(E1)
    gather1.finish()
    normalize(tok1, mixer_gain_ref)
    forward(A, 1)
    forward(B, 1)
    second_send(E2)
    forward(A, 2)
    forward(B, 2)
    first_wait(U, 3)
    first_wait(D0, 3)
    forward(A, 3)
    forward(B, 3)
    second_send(U0)
    second_send(U1)
    second_send(E0)
    second_wait(A)

    linear = jnp.dot(normed[...], all_rows(wa, slice(0, 256)), preferred_element_type=F32)
    spatial = jax.nn.gelu(linear[:, 128:256] * spatial_scale_ref[...])
    sq = spatial * spatial
    sq_high = sq.astype(BF16)
    sq_low = (sq - sq_high.astype(F32)).astype(BF16)
    ones = jnp.ones((8, 128), BF16)
    squares[tp] = nt_dot(ones, sq_high) + nt_dot(ones, sq_low)

    def square_copy(d, arriving=False):
        ref = squares.at[(tp + N_TP - d) % N_TP] if arriving else squares.at[tp]
        return remote(ref, ref, sq_send.at[0], sq_recv.at[d - 1], fs, (tp + d) % N_TP)

    for d in range(1, N_TP):
        square_copy(d).start()
    content = jax.nn.gelu(linear[:, 0:128] * content_scale_ref[...])
    gained = (spatial * spatial_gain_ref[...]).astype(BF16)
    causal = (
        lax.broadcasted_iota(jnp.int32, (BLOCK, BLOCK), 1)
        <= lax.broadcasted_iota(jnp.int32, (BLOCK, BLOCK), 0)
    )
    mixing = jnp.where(causal, mixing_ref[0].astype(F32), 0.0)
    bias = jnp.transpose(jnp.broadcast_to(bias_ref[...], (BLOCK, BLOCK)))
    for d in range(1, N_TP):
        square_copy(d, True).wait_recv()
    total_sq = squares[0]
    for t in range(1, N_TP):
        total_sq = total_sq + squares[t]
    row_scale = lax.rsqrt(total_sq[0:1] / (N_TP * 128) + EPSILON)
    gated_blocks = []
    for b in range(tokens_ref.shape[0] // BLOCK):
        rows = slice(b * BLOCK, (b + 1) * BLOCK)
        mixing_b = (mixing * row_scale[:, rows]).astype(BF16)
        mixed = jnp.dot(mixing_b, gained[rows], preferred_element_type=F32) + bias
        gated_blocks.append((content[rows] * mixed).astype(BF16))
    gated = jnp.concatenate(gated_blocks, axis=0)

    def project_blocks(k, dx):
        return tuple(
            nt_dot(gated, jnp.concatenate(plane_rows(wb, tp_of(dx, other), slice(0, 128)), axis=0))
            for other in (True, False))

    forward(U0, 1)
    second_wait(B)
    scatter1.begin(project_blocks)
    forward(U1, 1)
    scatter1.combine()
    forward(E0, 1)
    forward(U0, 2)
    middle = (tokens_ref[...].astype(F32) + scatter1.finish()).astype(BF16)
    tok2[tp] = middle
    gather2.begin()
    forward(U1, 2)
    forward(E0, 2)
    gather2.pass_on()
    forward(U0, 3)
    forward(E1, 1)
    gather2.far()
    forward(E2, 1)
    gather2.finish()
    forward(U1, 3)
    normalize(tok2, channel_gain_ref)
    forward(E0, 3)

    def up_tiles(k):
        for low in range(0, 512, 256):
            at = k * 512 + low
            up = jnp.dot(normed[...], all_rows(wu.at[k], slice(low, low + 256)), preferred_element_type=F32)
            up = jnp.maximum(up * up_scale_ref[:, at:at + 256], 0.0)
            hidden[:, at:at + 256] = (up * up).astype(BF16)

    second_wait(U0)
    up_tiles(0)
    forward(E1, 2)
    second_wait(U1)
    up_tiles(1)
    forward(E2, 2)

    natural = lax.broadcasted_iota(jnp.int32, (width, width), 0)
    split = lax.broadcasted_iota(jnp.int32, (width, width), 1)
    order = (
        natural == ((split % 128) // 16) * 32 + (split // 128) * 16 + split % 16
    ).astype(F32).astype(BF16)
    middle_split = jnp.dot(middle, order, preferred_element_type=F32)

    def down_pair(ref, k, dx):
        pieces = [r for other in (True, False) for r in plane_rows(ref.at[k], tp_of(dx, other), slice(0, 512))]
        return nt_dot(hidden[:, k * 512:(k + 1) * 512], jnp.concatenate(pieces, axis=0))

    def first_half(k, dx):
        both = down_pair(wd0, 0, dx) + down_pair(wd0, 1, dx)
        return both[:, 0:128], both[:, 128:256]

    def second_half(k, dx):
        both = partial[k] + down_pair(wd1, 1, dx)
        return both[:, 0:128], both[:, 128:256]

    second_wait(E0)
    scatter2.begin(first_half)
    forward(E1, 3)
    forward(E2, 3)
    scatter2.combine()
    second_wait(E1)
    for k, dx in enumerate(Scatter.order):
        partial[k] = down_pair(wd1, 0, dx)
    second_wait(E2)
    scatter3.begin(second_half)
    half0 = (middle_split[:, 0:128] + scatter2.finish()).astype(BF16)
    out0 = nt_dot(half0, order[:, 0:128])
    scatter3.combine()
    half1 = (middle_split[:, 128:256] + scatter3.finish()).astype(BF16)
    out_ref[...] = (out0 + nt_dot(half1, order[:, 128:256])).astype(BF16)
    store = pltpu.make_async_copy(out_ref, out_hbm, out_sem)
    store.start()

    for u in (A, B):
        ref = first_units[u].at[0, 0:7]
        remote(ref, ref, w1_send.at[u], w1_recv.at[u, 0], fs, tp_of(1, False)).wait_send()
    for u in (U, D0, D1):
        ref = first_units[u].at[:, 0, 0:7]
        remote(ref, ref, w1_send.at[u], w1_recv.at[u, 0], fs, tp_of(1, False)).wait_send()
    for u in range(7):
        ref = second_units[u].at[:, 0:7] if u == E0 else second_units[u].at[0:7]
        remote(ref, ref, w2_send.at[u], w2_recv.at[u, 0], fs, tp_of(1, False)).wait_send()
    gather1.drain()
    gather2.drain()
    scatter1.drain()
    scatter2.drain()
    scatter3.drain()
    remote(squares.at[0:7], squares.at[0:7], sq_send.at[0], sq_recv.at[0], fs, tp_of(1, False)).wait_send()
    store.wait()


def shards(
    tokens, mixer_gain, w_content, w_spatial, content_scale, spatial_scale, spatial_gain, block_mixing,
    block_bias, w_project, project_scale, channel_gain, w_up, up_scale, w_down, down_scale,
):
    rows, width = tokens.shape
    row = lambda v: v.reshape(1, -1)
    inputs = (
        tokens, row(mixer_gain), w_content, w_spatial, row(content_scale), row(spatial_scale),
        row(spatial_gain), block_mixing, block_bias, w_project.T, row(project_scale), row(channel_gain),
        w_up, row(up_scale), w_down.T, row(down_scale),
    )
    vmem = pltpu.VMEM
    dma = pltpu.SemaphoreType.DMA
    anywhere = pl.BlockSpec(memory_space=pl.ANY)
    return pl.pallas_call(
        layer_kernel,
        out_shape=jax.ShapeDtypeStruct((rows, width), BF16),
        in_specs=[anywhere] * N_INPUTS,
        out_specs=anywhere,
        scratch_shapes=[vmem(v.shape, v.dtype) for v in inputs] + [
            vmem((RING, RING, SLICE, 256), BF16),
            vmem((RING, RING, SLICE, 128), BF16),
            vmem((2, RING, RING, SLICE, 512), BF16),
            vmem((2, RING, RING, SLICE // 2, 512), BF16),
            vmem((2, RING, RING, SLICE // 2, 512), BF16),
            vmem((N_TP, rows, width), BF16),
            vmem((N_TP, rows, width), BF16),
            vmem((rows, N_TP * width), BF16),
            vmem((N_TP, 8, rows), F32),
            vmem((rows, w_up.shape[1]), BF16),
            vmem((4, rows, width), F32),
            vmem((rows, width), BF16),
            vmem((4, rows, 256), BF16), vmem((4, rows, 256), BF16), vmem((3, rows, 256), BF16),
            vmem((2, rows // 2, 256), BF16), vmem((2, rows, 256), BF16), vmem((4, rows, 256), F32),
            vmem((8, rows, 128), BF16), vmem((8, rows, 128), BF16), vmem((6, rows, 128), BF16),
            vmem((4, rows // 2, 128), BF16), vmem((4, rows, 128), BF16), vmem((8, rows, 128), F32),
            dma((N_INPUTS,)), dma, dma((5,)), dma((5, HOPS)), dma((7,)), dma((7, HOPS)),
            dma((2,)), dma((2, 8)), dma((3,)), dma((3, 10)), dma((1,)), dma((7,)),
        ],
        compiler_params=pltpu.CompilerParams(
            collective_id=0, has_side_effects=True, vmem_limit_bytes=56 * 1024 * 1024),
        name="layer",
    )(*inputs)


def solution(mesh):
    return jax.shard_map(
        shards,
        mesh=mesh,
        in_specs=(
            P("fs", "tp"), P(), P("fs", "tp"), P("fs", "tp"), P("tp"), P("tp"), P("tp"),
            P("tp", None, None), P("tp", None), P("tp", "fs"), P("fs"), P(), P("fs", "tp"), P("tp"),
            P("tp", "fs"), P("fs"),
        ),
        out_specs=P("fs", "tp"),
        check_vma=False,
    )
```

```python
import jax
import jax.numpy as jnp
from jax import lax
from jax.experimental import pallas as pl
from jax.experimental.pallas import tpu as pltpu
from jax.sharding import PartitionSpec as P

EPSILON = 1e-06
MESH = pl.DeviceIdType.MESH
F32 = jnp.float32
BF16 = jnp.bfloat16

RING = 8
HOPS = RING // 2
CHIPS_X = 4
N_TP = 2 * CHIPS_X
SLICE = 32
BLOCK = 128
N_INPUTS = 16


def nt_dot(left, right):
    return lax.dot_general(left, right, (((1,), (1,)), ((), ())), preferred_element_type=F32)


def layer_kernel(*refs):
    hbm = refs[:N_INPUTS]
    out_ref = refs[N_INPUTS]
    inputs = refs[N_INPUTS + 1:2 * N_INPUTS + 1]
    (
        tokens_ref, mixer_gain_ref, w_content_ref, w_spatial_ref, content_scale_ref, spatial_scale_ref,
        spatial_gain_ref, mixing_ref, bias_ref, w_project_ref, project_scale_ref, channel_gain_ref,
        w_up_ref, up_scale_ref, w_down_ref, down_scale_ref,
    ) = inputs
    (
        ws, wu, wd0, wd1, tok1, tok2, normed, squares, hidden,
        sib_out1, sib_in1, ring_out1, far_in1, near_in1, acc1,
        sib_out2, sib_in2, ring_out2, far_in2, near_in2, acc2,
        in_sem, w1_send, w1_recv, w2_send, w2_recv,
        ag_send, ag_recv, rs_send, rs_recv, sq_send, sq_recv,
    ) = refs[2 * N_INPUTS + 1:]
    fs, tp = lax.axis_index("fs"), lax.axis_index("tp")
    z, y = fs // RING, fs % RING
    x, core = tp // 2, tp % 2
    p = jnp.where(core == 0, y, z)
    q = jnp.where(core == 0, z, y)

    def fs_of(pp, qq):
        return jnp.where(core == 0, qq * RING + pp, pp * RING + qq)

    def tp_of(dx, other):
        c = (1 - core) if other else core
        return 2 * ((x + dx + CHIPS_X) % CHIPS_X) + c

    first_next = (fs_of((p + 1) % RING, q), fs_of((p + RING - 1) % RING, q))
    second_far = (fs_of(p, (q + 2) % RING), fs_of(p, (q + RING - 2) % RING))
    second_next = (fs_of(p, (q + 1) % RING), fs_of(p, (q + RING - 1) % RING))

    barrier = pltpu.get_barrier_semaphore()
    for to in tuple(fs_of((p + d) % RING, q) for d in range(1, RING)) + second_next + second_far:
        pl.semaphore_signal(barrier, inc=1, device_id=(to, tp), device_id_type=MESH)
    for d in range(1, N_TP):
        pl.semaphore_signal(barrier, inc=1, device_id=(fs, (tp + d) % N_TP), device_id_type=MESH)
    fetches = [pltpu.make_async_copy(hbm[i], inputs[i], in_sem.at[i]) for i in range(N_INPUTS)]
    for i in (2, 3, 9, 10, 0, 12, 14, 15, 1, 4, 5, 6, 7, 8, 11, 13):
        fetches[i].start()

    def remote(src, dst, ss, rs, to_fs, to_tp):
        return pltpu.make_async_remote_copy(
            src_ref=src, dst_ref=dst, send_sem=ss, recv_sem=rs,
            device_id=(to_fs, to_tp), device_id_type=MESH,
        )

    eye = (
        lax.broadcasted_iota(jnp.int32, (SLICE, SLICE), 0)
        == lax.broadcasted_iota(jnp.int32, (SLICE, SLICE), 1)
    )

    def scaled(w, scale):
        column = jnp.sum(jnp.where(eye, scale, 0.0), axis=1, keepdims=True)
        return (w.astype(BF16).astype(F32) * column).astype(BF16)

    for i in (2, 3, 9, 10):
        fetches[i].wait()
    ws[q, 0, :, 0:128] = w_content_ref[...].astype(BF16)
    ws[q, 0, :, 128:256] = w_spatial_ref[...].astype(BF16)
    ws[q, 0, :, 256:384] = scaled(w_project_ref[...], project_scale_ref[...])
    for i in (0, 12, 14, 15):
        fetches[i].wait()
    tok1[tp] = tokens_ref[...]
    down = scaled(w_down_ref[...], down_scale_ref[...])
    for k in range(2):
        cols = slice(k * 512, (k + 1) * 512)
        wu[k, q, 0] = w_up_ref[:, cols].astype(BF16)
        wd0[k, q, 0] = down[0:16, cols]
        wd1[k, q, 0] = down[16:32, cols]
    pl.semaphore_wait(barrier, RING - 1 + 4 + N_TP - 1)

    S, U, D0, D1 = range(4)
    units = (ws, wu, wd0, wd1)

    def first_copy(u, src, dst, to, sem, part=None):
        if u == S:
            src_ref, dst_ref = ws.at[q, src], ws.at[q, dst]
        else:
            lead = slice(None) if part is None else part
            src_ref, dst_ref = units[u].at[lead, q, src], units[u].at[lead, q, dst]
        return remote(src_ref, dst_ref, w1_send.at[u], w1_recv.at[u, sem], to, tp)

    places = {0: 0, 1: 1, -1: 2, 2: 3, -2: 4, 3: 5, -3: 6, 4: 7, -4: 7}

    def first_send(u, step):
        for way in range(2):
            sign = 1 if way else -1
            first_copy(u, places[sign * step], places[sign * (step + 1)], first_next[way], step,
                       way if step == HOPS - 1 else None).start()

    def small_send():
        for d in (1, -1, 2, -2, 3, -3, 4):
            first_copy(S, 0, places[-d], fs_of((p + d + RING) % RING, q), 0 if abs(d) == 1 else 1).start()

    def small_wait(sem):
        ref = ws.at[0, 0:2] if sem == 0 else ws.at[0, 0:5]
        remote(ref, ref, w1_send.at[S], w1_recv.at[S, sem], first_next[0], tp).wait_recv()

    def first_wait(u, distance):
        n = 1 if distance == HOPS else 2
        ref = units[u].at[:, 0, 0:n]
        remote(ref, ref, w1_send.at[u], w1_recv.at[u, distance - 1], first_next[0], tp).wait_recv()

    def first_forward(u, step):
        first_wait(u, step)
        first_send(u, step)

    Sa, Sb, Ua, Ub, D0a, D0b, D1a, D1b = range(8)

    def group(g, at, lead=slice(None)):
        shards_of = pl.ds(0, 3) if g % 2 == 0 else pl.ds(3, 5)
        return ws.at[at, shards_of] if g < 2 else units[g // 2].at[lead, at, shards_of]

    def second_copy(g, way, step):
        at = (q + (step if way else -step) + RING) % RING
        ref = group(g, at)
        if step == HOPS - 1:
            ref = ref.at[:, pl.ds(way * (SLICE // 2), SLICE // 2)] if g < 2 else group(g, at, way)
        return remote(ref, ref, w2_send.at[g], w2_recv.at[g, step], second_next[way], tp)

    def far_copy(g, way, step):
        at = (q + (2 * step if way else -2 * step) + RING) % RING
        ref = group(g, at)
        if step == 1:
            ref = ref.at[:, pl.ds(way * (SLICE // 2), SLICE // 2)]
        return remote(ref, ref, w2_send.at[g], w2_recv.at[g, 2 * step + 1], second_far[way], tp)

    def two_stage(g, step):
        if step == 1:
            second_wait(g, 1)
        for way in range(2):
            far_copy(g, way, step).start()
        for way in range(2):
            second_copy(g, way, 2 * step).start()

    def two_stage_wait(g):
        for step in (0, 2, 3):
            second_wait(g, step)

    def second_send(g, step=0):
        for way in range(2):
            second_copy(g, way, step).start()

    def second_wait(g, step=HOPS - 1):
        ref = group(g, 0) if step == HOPS - 1 else group(g, pl.ds(0, 2))
        remote(ref, ref, w2_send.at[g], w2_recv.at[g, step], second_next[0], tp).wait_recv()

    def forward(g, step):
        second_wait(g, step - 1)
        second_send(g, step)

    half = tokens_ref.shape[0] // 2

    class Gather:
        def __init__(self, buf, n):
            self.buf, self.n = buf, n

        def copy(self, k, arriving=False):
            dx = (0, -1, 1, 2, 0, 0, -1, 1)[k]
            if arriving and k >= 4:
                dx = (-1, 1, -2, 2)[k - 4]
            ref = self.buf.at[tp_of(dx, arriving and k < 4)]
            if k >= 6:
                ref = ref.at[pl.ds((k - 6) * half, half)]
            to = tp_of(0, True) if k < 4 else tp_of((1, -1)[k % 2], False)
            return remote(ref, ref, ag_send.at[self.n], ag_recv.at[self.n, k], fs, to)

        def begin(self):
            for k in (4, 5, 0):
                self.copy(k).start()

        def pass_on(self):
            for k in range(2):
                self.copy(4 + k, True).wait_recv()
                self.copy(6 + k).start()
                self.copy(1 + k).start()

        def far(self):
            for k in range(2):
                self.copy(6 + k, True).wait_recv()
            self.copy(3).start()

        def finish(self):
            for k in range(4):
                self.copy(k, True).wait_recv()

        def drain(self):
            ref = self.buf.at[0:7]
            remote(ref, ref, ag_send.at[self.n], ag_recv.at[self.n, 0], fs, tp_of(1, False)).wait_send()

    class Scatter:
        order = (2, 1, -1, 0)

        def __init__(self, n, bufs, bytes_ref):
            self.n, self.bytes_ref = n, bytes_ref
            self.sib_out, self.sib_in, self.ring_out, self.far_in, self.near_in, self.acc = bufs

        def copy(self, src, dst, k, to):
            return remote(src, dst, rs_send.at[self.n], rs_recv.at[self.n, k], fs, to)

        def across(self, k):
            return self.copy(self.sib_out.at[k], self.sib_in.at[k], k, tp_of(0, True))

        def far(self, way):
            return self.copy(self.ring_out.at[0, pl.ds(way * half, half)], self.far_in.at[way], 4 + way,
                             tp_of((1, -1)[way], False))

        def near(self, way, part):
            rows = pl.ds(part * half, half)
            return self.copy(self.ring_out.at[1 + way, rows], self.near_in.at[way, rows], 6 + 2 * way + part,
                             tp_of((1, -1)[way], False))

        def begin(self, blocks_of):
            for k, dx in enumerate(self.order):
                across, own = blocks_of(k, dx)
                self.sib_out[k] = across.astype(BF16)
                self.across(k).start()
                self.acc[k] = own
                if k > 0:
                    self.own(k - 1)

        def own(self, k):
            self.across(k).wait_recv()
            value = self.acc[k] + self.sib_in[k].astype(F32)
            if k == 0:
                self.ring_out[0] = value.astype(BF16)
                self.far(0).start()
                self.far(1).start()
            else:
                self.acc[k] = value
                if k < 3:
                    part = 2 - k
                    rows = slice(part * half, (part + 1) * half)
                    self.ring_out[k, rows] = value[rows].astype(BF16)
                    self.near(k - 1, part).start()

        def combine(self):
            for way in range(2):
                self.far(way).wait_recv()
                rows = slice(way * half, (way + 1) * half)
                self.ring_out[1 + way, rows] = (
                    self.acc[1 + way, rows] + self.far_in[way].astype(F32)).astype(BF16)
                self.near(way, way).start()

        def finish(self):
            self.own(3)
            for way in range(2):
                for part in range(2):
                    self.near(way, part).wait_recv()
            return self.acc[3] + self.near_in[0].astype(F32) + self.near_in[1].astype(F32)

        def drain(self):
            remote(self.bytes_ref, self.bytes_ref, rs_send.at[self.n], rs_recv.at[self.n, 0], fs,
                   tp_of(1, False)).wait_send()

    width = tokens_ref.shape[1]

    def normalize(buf, gain_ref):
        total = None
        for t in range(N_TP):
            v = buf[t].astype(F32)
            s = jnp.sum(v * v, axis=1, keepdims=True)
            total = s if total is None else total + s
        r = lax.rsqrt(total / (N_TP * width) + EPSILON)
        for t in range(N_TP):
            cols = slice(t * width, (t + 1) * width)
            normed[:, cols] = (buf[t].astype(F32) * r * gain_ref[:, cols]).astype(BF16)

    def plane_rows(ref, zz, cols):
        rows = []
        for j in range(RING):
            first, second = jnp.where(core == 0, j, zz), jnp.where(core == 0, zz, j)
            d = (first - p + RING) % RING
            at = jnp.where((d >= 1) & (d <= HOPS), 2 * d - 1, (2 * (RING - d)) % (2 * RING))
            rows.append(ref[second, at, :, cols])
        return rows

    def all_rows(ref, cols):
        return jnp.concatenate([r for zz in range(RING) for r in plane_rows(ref, zz, cols)], axis=0)

    def set_of(*bufs, low=None):
        return bufs if low is None else tuple(b.at[pl.ds(low * (b.shape[0] // 2), b.shape[0] // 2)] for b in bufs)

    gather1, gather2 = Gather(tok1, 0), Gather(tok2, 1)
    bufs2 = (sib_out2, sib_in2, ring_out2, far_in2, near_in2, acc2)
    scatter1 = Scatter(0, (sib_out1, sib_in1, ring_out1, far_in1, near_in1, acc1), tok1.at[0:7])
    scatter2 = Scatter(1, set_of(*bufs2, low=0), sib_out2.at[0:7])
    scatter3 = Scatter(2, set_of(*bufs2, low=1), sib_out2.at[0:7])

    small_send()
    gather1.begin()
    first_send(U, 0)
    first_send(D0, 0)
    first_send(D1, 0)
    small_wait(0)
    two_stage(Sa, 0)
    first_forward(U, 1)
    first_forward(D0, 1)
    first_forward(D1, 1)
    small_wait(1)
    two_stage(Sb, 0)
    gather1.pass_on()
    first_forward(U, 2)
    second_send(Ua)
    first_forward(D0, 2)
    first_forward(D1, 2)
    two_stage(Sa, 1)
    second_send(D0a)
    gather1.far()
    first_forward(U, 3)
    first_forward(D0, 3)
    first_forward(D1, 3)
    two_stage(Sb, 1)
    second_send(D1a)
    forward(Ua, 1)
    for i in (1, 4, 5, 6, 7, 8, 11, 13):
        fetches[i].wait()
    gather1.finish()
    normalize(tok1, mixer_gain_ref)
    first_wait(U, 4)
    second_send(Ub)
    first_wait(D0, 4)
    second_send(D0b)
    first_wait(D1, 4)
    second_send(D1b)
    two_stage_wait(Sa)
    two_stage_wait(Sb)

    linear = jnp.dot(normed[...], all_rows(ws, slice(0, 256)), preferred_element_type=F32)
    spatial = jax.nn.gelu(linear[:, 128:256] * spatial_scale_ref[...])
    sq = spatial * spatial
    sq_high = sq.astype(BF16)
    sq_low = (sq - sq_high.astype(F32)).astype(BF16)
    ones = jnp.ones((8, 128), BF16)
    squares[tp] = nt_dot(ones, sq_high) + nt_dot(ones, sq_low)

    def square_copy(d, arriving=False):
        ref = squares.at[(tp + N_TP - d) % N_TP] if arriving else squares.at[tp]
        return remote(ref, ref, sq_send.at[0], sq_recv.at[d - 1], fs, (tp + d) % N_TP)

    for d in range(1, N_TP):
        square_copy(d).start()
    content = jax.nn.gelu(linear[:, 0:128] * content_scale_ref[...])
    gained = (spatial * spatial_gain_ref[...]).astype(BF16)
    causal = (
        lax.broadcasted_iota(jnp.int32, (BLOCK, BLOCK), 1)
        <= lax.broadcasted_iota(jnp.int32, (BLOCK, BLOCK), 0)
    )
    mixing = jnp.where(causal, mixing_ref[0].astype(F32), 0.0)
    bias = jnp.transpose(jnp.broadcast_to(bias_ref[...], (BLOCK, BLOCK)))
    forward(D0a, 1)
    forward(D1a, 1)
    for d in range(1, N_TP):
        square_copy(d, True).wait_recv()
    total_sq = squares[0]
    for t in range(1, N_TP):
        total_sq = total_sq + squares[t]
    row_scale = lax.rsqrt(total_sq[0:1] / (N_TP * 128) + EPSILON)
    gated_blocks = []
    for b in range(tokens_ref.shape[0] // BLOCK):
        rows = slice(b * BLOCK, (b + 1) * BLOCK)
        mixing_b = (mixing * row_scale[:, rows]).astype(BF16)
        mixed = jnp.dot(mixing_b, gained[rows], preferred_element_type=F32) + bias
        gated_blocks.append((content[rows] * mixed).astype(BF16))
    gated = jnp.concatenate(gated_blocks, axis=0)

    def project_blocks(k, dx):
        return tuple(
            nt_dot(gated, jnp.concatenate(plane_rows(ws, tp_of(dx, other), slice(256, 384)), axis=0))
            for other in (True, False))

    forward(Ub, 1)
    scatter1.begin(project_blocks)
    forward(D0b, 1)
    forward(Ua, 2)
    forward(D1b, 1)
    scatter1.combine()
    forward(D0a, 2)
    forward(Ub, 2)
    middle = (tokens_ref[...].astype(F32) + scatter1.finish()).astype(BF16)
    tok2[tp] = middle
    gather2.begin()
    forward(D0b, 2)
    forward(Ua, 3)
    forward(D1a, 2)
    forward(D1b, 2)
    forward(D0a, 3)
    gather2.pass_on()
    forward(Ub, 3)
    gather2.far()
    forward(D0b, 3)
    gather2.finish()
    forward(D1a, 3)
    forward(D1b, 3)
    normalize(tok2, channel_gain_ref)

    def up_tiles(k):
        for low in range(0, 512, 256):
            at = k * 512 + low
            up = jnp.dot(normed[...], all_rows(wu.at[k], slice(low, low + 256)), preferred_element_type=F32)
            up = jnp.maximum(up * up_scale_ref[:, at:at + 256], 0.0)
            hidden[:, at:at + 256] = (up * up).astype(BF16)

    second_wait(Ua)
    second_wait(Ub)
    up_tiles(0)
    up_tiles(1)

    natural = lax.broadcasted_iota(jnp.int32, (width, width), 0)
    split = lax.broadcasted_iota(jnp.int32, (width, width), 1)
    order = (
        natural == ((split % 128) // 16) * 32 + (split // 128) * 16 + split % 16
    ).astype(F32).astype(BF16)
    middle_split = jnp.dot(middle, order, preferred_element_type=F32)

    def down_pair(ref, k, dx):
        pieces = [r for other in (True, False) for r in plane_rows(ref.at[k], tp_of(dx, other), slice(0, 512))]
        return nt_dot(hidden[:, k * 512:(k + 1) * 512], jnp.concatenate(pieces, axis=0))

    def down_half(ref):
        def blocks(k, dx):
            both = down_pair(ref, 0, dx) + down_pair(ref, 1, dx)
            return both[:, 0:128], both[:, 128:256]

        return blocks

    second_wait(D0a)
    second_wait(D0b)
    scatter2.begin(down_half(wd0))
    second_wait(D1a)
    second_wait(D1b)
    scatter3.begin(down_half(wd1))
    scatter2.combine()
    scatter3.combine()
    half0 = (middle_split[:, 0:128] + scatter2.finish()).astype(BF16)
    out0 = nt_dot(half0, order[:, 0:128])
    half1 = (middle_split[:, 128:256] + scatter3.finish()).astype(BF16)
    out_ref[...] = (out0 + nt_dot(half1, order[:, 128:256])).astype(BF16)

    for u in range(4):
        ref = ws.at[0, 0:7] if u == S else units[u].at[:, 0, 0:7]
        remote(ref, ref, w1_send.at[u], w1_recv.at[u, 0], fs, tp_of(1, False)).wait_send()
    for g in range(8):
        ref = group(g, pl.ds(0, 7))
        remote(ref, ref, w2_send.at[g], w2_recv.at[g, 0], fs, tp_of(1, False)).wait_send()
    gather1.drain()
    gather2.drain()
    scatter1.drain()
    scatter2.drain()
    scatter3.drain()
    remote(squares.at[0:7], squares.at[0:7], sq_send.at[0], sq_recv.at[0], fs, tp_of(1, False)).wait_send()


def shards(
    tokens, mixer_gain, w_content, w_spatial, content_scale, spatial_scale, spatial_gain, block_mixing,
    block_bias, w_project, project_scale, channel_gain, w_up, up_scale, w_down, down_scale,
):
    rows, width = tokens.shape
    row = lambda v: v.reshape(1, -1)
    inputs = (
        tokens, row(mixer_gain), w_content, w_spatial, row(content_scale), row(spatial_scale),
        row(spatial_gain), block_mixing, block_bias, w_project.T, row(project_scale), row(channel_gain),
        w_up, row(up_scale), w_down.T, row(down_scale),
    )
    vmem = pltpu.VMEM
    dma = pltpu.SemaphoreType.DMA
    anywhere = pl.BlockSpec(memory_space=pl.ANY)
    return pl.pallas_call(
        layer_kernel,
        out_shape=pltpu.VMEM((rows, width), BF16),
        in_specs=[anywhere] * N_INPUTS,
        out_specs=pl.BlockSpec(memory_space=pltpu.VMEM),
        scratch_shapes=[vmem(v.shape, v.dtype) for v in inputs] + [
            vmem((RING, RING, SLICE, 384), BF16),
            vmem((2, RING, RING, SLICE, 512), BF16),
            vmem((2, RING, RING, SLICE // 2, 512), BF16),
            vmem((2, RING, RING, SLICE // 2, 512), BF16),
            vmem((N_TP, rows, width), BF16),
            vmem((N_TP, rows, width), BF16),
            vmem((rows, N_TP * width), BF16),
            vmem((N_TP, 8, rows), F32),
            vmem((rows, w_up.shape[1]), BF16),
            vmem((4, rows, 256), BF16), vmem((4, rows, 256), BF16), vmem((3, rows, 256), BF16),
            vmem((2, rows // 2, 256), BF16), vmem((2, rows, 256), BF16), vmem((4, rows, 256), F32),
            vmem((8, rows, 128), BF16), vmem((8, rows, 128), BF16), vmem((6, rows, 128), BF16),
            vmem((4, rows // 2, 128), BF16), vmem((4, rows, 128), BF16), vmem((8, rows, 128), F32),
            dma((N_INPUTS,)), dma((4,)), dma((4, HOPS)), dma((8,)), dma((8, HOPS)),
            dma((2,)), dma((2, 8)), dma((3,)), dma((3, 10)), dma((1,)), dma((7,)),
        ],
        compiler_params=pltpu.CompilerParams(
            collective_id=0, has_side_effects=True, vmem_limit_bytes=56 * 1024 * 1024),
        name="layer",
    )(*inputs)


def solution(mesh):
    return jax.shard_map(
        shards,
        mesh=mesh,
        in_specs=(
            P("fs", "tp"), P(), P("fs", "tp"), P("fs", "tp"), P("tp"), P("tp"), P("tp"),
            P("tp", None, None), P("tp", None), P("tp", "fs"), P("fs"), P(), P("fs", "tp"), P("tp"),
            P("tp", "fs"), P("fs"),
        ),
        out_specs=P("fs", "tp"),
        check_vma=False,
    )
```

```python
import jax
import jax.numpy as jnp
from jax import lax
from jax.experimental import pallas as pl
from jax.experimental.pallas import tpu as pltpu
from jax.sharding import PartitionSpec as P

EPSILON = 1e-06
MESH = pl.DeviceIdType.MESH
F32 = jnp.float32
BF16 = jnp.bfloat16

RING = 8
HOPS = RING // 2
CHIPS_X = 4
N_TP = 2 * CHIPS_X
SLICE = 32
BLOCK = 128
N_INPUTS = 16


def nt_dot(left, right):
    return lax.dot_general(left, right, (((1,), (1,)), ((), ())), preferred_element_type=F32)


def layer_kernel(*refs):
    hbm = refs[:N_INPUTS]
    out_ref = refs[N_INPUTS]
    inputs = refs[N_INPUTS + 1:2 * N_INPUTS + 1]
    (
        tokens_ref, mixer_gain_ref, w_content_ref, w_spatial_ref, content_scale_ref, spatial_scale_ref,
        spatial_gain_ref, mixing_ref, bias_ref, w_project_ref, project_scale_ref, channel_gain_ref,
        w_up_ref, up_scale_ref, w_down_ref, down_scale_ref,
    ) = inputs
    (
        wp, wc, wu, wd0, wd1, tok1, tok2, normed, squares, hidden, up_acc,
        sib_out1, sib_in1, ring_out1, far_in1, near_in1, acc1,
        sib_out2, sib_in2, ring_out2, far_in2, near_in2, acc2,
        in_sem, w1_send, w1_recv, w2_send, w2_recv,
        ag_send, ag_recv, rs_send, rs_recv, sq_send, sq_recv,
    ) = refs[2 * N_INPUTS + 1:]
    fs, tp = lax.axis_index("fs"), lax.axis_index("tp")
    z, y = fs // RING, fs % RING
    x, core = tp // 2, tp % 2
    p = jnp.where(core == 0, y, z)
    q = jnp.where(core == 0, z, y)

    def fs_of(pp, qq):
        return jnp.where(core == 0, qq * RING + pp, pp * RING + qq)

    def tp_of(dx, other):
        c = (1 - core) if other else core
        return 2 * ((x + dx + CHIPS_X) % CHIPS_X) + c

    first_next = (fs_of((p + 1) % RING, q), fs_of((p + RING - 1) % RING, q))
    second_next = (fs_of(p, (q + 1) % RING), fs_of(p, (q + RING - 1) % RING))

    barrier = pltpu.get_barrier_semaphore()
    for to in tuple(fs_of((p + d) % RING, q) for d in range(1, RING)) + second_next:
        pl.semaphore_signal(barrier, inc=1, device_id=(to, tp), device_id_type=MESH)
    for d in range(1, N_TP):
        pl.semaphore_signal(barrier, inc=1, device_id=(fs, (tp + d) % N_TP), device_id_type=MESH)
    fetches = [pltpu.make_async_copy(hbm[i], inputs[i], in_sem.at[i]) for i in range(N_INPUTS)]
    for i in (2, 3, 9, 10, 0, 12, 14, 15, 1, 4, 5, 6, 7, 8, 11, 13):
        fetches[i].start()

    def remote(src, dst, ss, rs, to_fs, to_tp):
        return pltpu.make_async_remote_copy(
            src_ref=src, dst_ref=dst, send_sem=ss, recv_sem=rs,
            device_id=(to_fs, to_tp), device_id_type=MESH,
        )

    eye = (
        lax.broadcasted_iota(jnp.int32, (SLICE, SLICE), 0)
        == lax.broadcasted_iota(jnp.int32, (SLICE, SLICE), 1)
    )

    def scaled(w, scale):
        column = jnp.sum(jnp.where(eye, scale, 0.0), axis=1, keepdims=True)
        return (w.astype(BF16).astype(F32) * column).astype(BF16)

    for i in (2, 3, 9, 10):
        fetches[i].wait()
    wp[q, 0] = w_spatial_ref[...].astype(BF16)
    wc[q, 0, :, 0:128] = w_content_ref[...].astype(BF16)
    wc[q, 0, :, 128:256] = scaled(w_project_ref[...], project_scale_ref[...])
    for i in (0, 12, 14, 15):
        fetches[i].wait()
    tok1[tp] = tokens_ref[...]
    down = scaled(w_down_ref[...], down_scale_ref[...])
    for k in range(2):
        cols = slice(k * 512, (k + 1) * 512)
        wu[k, q, 0] = w_up_ref[:, cols].astype(BF16)
        wd0[k, q, 0] = down[0:16, cols]
        wd1[k, q, 0] = down[16:32, cols]
    pl.semaphore_wait(barrier, RING - 1 + 2 + N_TP - 1)

    SP, SC, U, D0, D1 = range(5)
    units = (wp, wc, wu, wd0, wd1)

    def first_copy(u, src, dst, to, sem, part=None):
        if u <= SC:
            src_ref, dst_ref = units[u].at[q, src], units[u].at[q, dst]
        else:
            lead = slice(None) if part is None else part
            src_ref, dst_ref = units[u].at[lead, q, src], units[u].at[lead, q, dst]
        return remote(src_ref, dst_ref, w1_send.at[u], w1_recv.at[u, sem], to, tp)

    places = {0: 0, 1: 1, -1: 2, 2: 3, -2: 4, 3: 5, -3: 6, 4: 7, -4: 7}

    def first_send(u, step):
        for way in range(2):
            sign = 1 if way else -1
            first_copy(u, places[sign * step], places[sign * (step + 1)], first_next[way], step,
                       way if step == HOPS - 1 else None).start()

    def small_send(u):
        for d in (1, -1, 2, -2, 3, -3, 4):
            first_copy(u, 0, places[-d], fs_of((p + d + RING) % RING, q), 0 if abs(d) == 1 else 1).start()

    def small_wait(u, sem):
        ref = units[u].at[0, 0:2] if sem == 0 else units[u].at[0, 0:5]
        remote(ref, ref, w1_send.at[u], w1_recv.at[u, sem], first_next[0], tp).wait_recv()

    def first_wait(u, distance=HOPS):
        n = 1 if distance == HOPS else 2
        ref = units[u].at[:, 0, 0:n]
        remote(ref, ref, w1_send.at[u], w1_recv.at[u, distance - 1], first_next[0], tp).wait_recv()

    def first_forward(u, step):
        first_wait(u, step)
        first_send(u, step)

    SPa, SPb, SCa, SCb, Ua, Ub, D0a, D0b, D1a, D1b = range(10)
    SMALL = 4

    def group(g, at, lead=slice(None)):
        shards_of = pl.ds(0, 3) if g % 2 == 0 else pl.ds(3, 5)
        return units[g // 2].at[at, shards_of] if g < SMALL else units[g // 2].at[lead, at, shards_of]

    def second_copy(g, way, step):
        at = (q + (step if way else -step) + RING) % RING
        ref = group(g, at)
        if step == HOPS - 1:
            ref = ref.at[:, pl.ds(way * (SLICE // 2), SLICE // 2)] if g < SMALL else group(g, at, way)
        return remote(ref, ref, w2_send.at[g], w2_recv.at[g, step], second_next[way], tp)

    def second_send(g, step=0):
        for way in range(2):
            second_copy(g, way, step).start()

    def second_wait(g, step=HOPS - 1):
        ref = group(g, 0) if step == HOPS - 1 else group(g, pl.ds(0, 2))
        remote(ref, ref, w2_send.at[g], w2_recv.at[g, step], second_next[0], tp).wait_recv()

    def forward(g, step):
        second_wait(g, step - 1)
        second_send(g, step)

    half = tokens_ref.shape[0] // 2

    class Gather:
        def __init__(self, buf, n):
            self.buf, self.n = buf, n

        def copy(self, k, arriving=False):
            dx = (0, -1, 1, 2, 0, 0, 0, 0, -1, 1)[k]
            if arriving and k >= 4:
                dx = (-1, 1, -1, 1, -2, 2)[k - 4]
            ref = self.buf.at[tp_of(dx, arriving and k < 4)]
            if k >= 4:
                ref = ref.at[pl.ds((k % 2 if k // 2 != 3 else 1 - k % 2) * half, half)]
            to = tp_of(0, True) if k < 4 else tp_of((1, -1)[k % 2], False)
            return remote(ref, ref, ag_send.at[self.n], ag_recv.at[self.n, k], fs, to)

        def begin(self):
            for k in (4, 5, 6, 7, 0):
                self.copy(k).start()

        def pass_on(self):
            for k in range(2):
                self.copy(4 + k, True).wait_recv()
                self.copy(8 + k).start()

        def near(self):
            for k in range(2):
                self.copy(6 + k, True).wait_recv()
                self.copy(1 + k).start()

        def far(self):
            for k in range(2):
                self.copy(8 + k, True).wait_recv()
            self.copy(3).start()

        def wait(self, *which):
            for k in which:
                self.copy(k, True).wait_recv()

        def drain(self):
            ref = self.buf.at[0:7]
            remote(ref, ref, ag_send.at[self.n], ag_recv.at[self.n, 0], fs, tp_of(1, False)).wait_send()

    class Scatter:
        order = (2, 1, -1, 0)

        def __init__(self, n, bufs, bytes_ref):
            self.n, self.bytes_ref = n, bytes_ref
            self.sib_out, self.sib_in, self.ring_out, self.far_in, self.near_in, self.acc = bufs

        def copy(self, src, dst, k, to):
            return remote(src, dst, rs_send.at[self.n], rs_recv.at[self.n, k], fs, to)

        def across(self, k):
            return self.copy(self.sib_out.at[k], self.sib_in.at[k], k, tp_of(0, True))

        def far(self, way):
            return self.copy(self.ring_out.at[0, pl.ds(way * half, half)], self.far_in.at[way], 4 + way,
                             tp_of((1, -1)[way], False))

        def near(self, way, part):
            rows = pl.ds(part * half, half)
            return self.copy(self.ring_out.at[1 + way, rows], self.near_in.at[way, rows], 6 + 2 * way + part,
                             tp_of((1, -1)[way], False))

        def begin(self, blocks_of):
            for k, dx in enumerate(self.order):
                across, own = blocks_of(k, dx)
                self.sib_out[k] = across.astype(BF16)
                self.across(k).start()
                self.acc[k] = own
                if k > 0:
                    self.own(k - 1)

        def own(self, k):
            self.across(k).wait_recv()
            value = self.acc[k] + self.sib_in[k].astype(F32)
            if k == 0:
                self.ring_out[0] = value.astype(BF16)
                self.far(0).start()
                self.far(1).start()
            else:
                self.acc[k] = value
                if k < 3:
                    part = 2 - k
                    rows = slice(part * half, (part + 1) * half)
                    self.ring_out[k, rows] = value[rows].astype(BF16)
                    self.near(k - 1, part).start()

        def combine(self):
            for way in range(2):
                self.far(way).wait_recv()
                rows = slice(way * half, (way + 1) * half)
                self.ring_out[1 + way, rows] = (
                    self.acc[1 + way, rows] + self.far_in[way].astype(F32)).astype(BF16)
                self.near(way, way).start()

        def finish(self):
            self.own(3)
            for way in range(2):
                for part in range(2):
                    self.near(way, part).wait_recv()
            return self.acc[3] + self.near_in[0].astype(F32) + self.near_in[1].astype(F32)

        def drain(self):
            remote(self.bytes_ref, self.bytes_ref, rs_send.at[self.n], rs_recv.at[self.n, 0], fs,
                   tp_of(1, False)).wait_send()

    width = tokens_ref.shape[1]

    def normalize():
        total = None
        for t in range(N_TP):
            v = tok1[t].astype(F32)
            s = jnp.sum(v * v, axis=1, keepdims=True)
            total = s if total is None else total + s
        r = lax.rsqrt(total / (N_TP * width) + EPSILON)
        for t in range(N_TP):
            cols = slice(t * width, (t + 1) * width)
            normed[:, cols] = (tok1[t].astype(F32) * r * mixer_gain_ref[:, cols]).astype(BF16)

    def plane_rows(ref, zz, cols):
        rows = []
        for j in range(RING):
            first, second = jnp.where(core == 0, j, zz), jnp.where(core == 0, zz, j)
            d = (first - p + RING) % RING
            at = jnp.where((d >= 1) & (d <= HOPS), 2 * d - 1, (2 * (RING - d)) % (2 * RING))
            rows.append(ref[second, at, :, cols])
        return rows

    def all_rows(ref, cols):
        return jnp.concatenate([r for zz in range(RING) for r in plane_rows(ref, zz, cols)], axis=0)

    def set_of(*bufs, low=None):
        return bufs if low is None else tuple(b.at[pl.ds(low * (b.shape[0] // 2), b.shape[0] // 2)] for b in bufs)

    gather1, gather2 = Gather(tok1, 0), Gather(tok2, 1)
    bufs2 = (sib_out2, sib_in2, ring_out2, far_in2, near_in2, acc2)
    scatter1 = Scatter(0, (sib_out1, sib_in1, ring_out1, far_in1, near_in1, acc1), tok1.at[0:7])
    scatter2 = Scatter(1, set_of(*bufs2, low=0), sib_out2.at[0:7])
    scatter3 = Scatter(2, set_of(*bufs2, low=1), sib_out2.at[0:7])

    value = {}

    def square_copy(d, arriving=False):
        ref = squares.at[(tp + N_TP - d) % N_TP] if arriving else squares.at[tp]
        return remote(ref, ref, sq_send.at[0], sq_recv.at[d - 1], fs, (tp + d) % N_TP)

    def spatial_branch():
        linear = jnp.dot(normed[...], all_rows(wp, slice(0, 128)), preferred_element_type=F32)
        spatial = jax.nn.gelu(linear * spatial_scale_ref[...])
        sq = spatial * spatial
        sq_high = sq.astype(BF16)
        sq_low = (sq - sq_high.astype(F32)).astype(BF16)
        ones = jnp.ones((8, 128), BF16)
        squares[tp] = nt_dot(ones, sq_high) + nt_dot(ones, sq_low)
        for d in range(1, N_TP):
            square_copy(d).start()
        value["gained"] = (spatial * spatial_gain_ref[...]).astype(BF16)

    def content_branch():
        linear = jnp.dot(normed[...], all_rows(wc, slice(0, 128)), preferred_element_type=F32)
        value["content"] = jax.nn.gelu(linear * content_scale_ref[...])
        causal = (
            lax.broadcasted_iota(jnp.int32, (BLOCK, BLOCK), 1)
            <= lax.broadcasted_iota(jnp.int32, (BLOCK, BLOCK), 0)
        )
        value["mixing"] = jnp.where(causal, mixing_ref[0].astype(F32), 0.0)
        value["bias"] = jnp.transpose(jnp.broadcast_to(bias_ref[...], (BLOCK, BLOCK)))

    def square_wait():
        for d in range(1, N_TP):
            square_copy(d, True).wait_recv()

    def mix():
        total_sq = squares[0]
        for t in range(1, N_TP):
            total_sq = total_sq + squares[t]
        row_scale = lax.rsqrt(total_sq[0:1] / (N_TP * 128) + EPSILON)
        gated = []
        for b in range(tokens_ref.shape[0] // BLOCK):
            rows = slice(b * BLOCK, (b + 1) * BLOCK)
            mixing_b = (value["mixing"] * row_scale[:, rows]).astype(BF16)
            mixed = jnp.dot(mixing_b, value["gained"][rows], preferred_element_type=F32) + value["bias"]
            gated.append((value["content"][rows] * mixed).astype(BF16))
        value["gated"] = jnp.concatenate(gated, axis=0)

    def project_blocks(k, dx):
        return tuple(
            nt_dot(value["gated"], jnp.concatenate(plane_rows(wc, tp_of(dx, other), slice(128, 256)), axis=0))
            for other in (True, False))

    def middle():
        value["middle"] = (tokens_ref[...].astype(F32) + scatter1.finish()).astype(BF16)
        tok2[tp] = value["middle"]
        gather2.begin()

    def up_part(dxs, first=False):
        blocks = [tp_of(dx, other) for dx in dxs for other in (False, True)]
        terms = []
        for t in blocks:
            v = tok2[t].astype(F32)
            s = jnp.sum(v * v, axis=1, keepdims=True)
            value["sum"] = s if first and not terms else value["sum"] + s
            gain = channel_gain_ref[:, pl.ds(pl.multiple_of(t * width, 128), width)]
            terms.append((v * gain).astype(BF16))
        left = jnp.concatenate(terms, axis=1)
        for k in range(2):
            for low in range(0, 512, 256):
                cols = slice(low, low + 256)
                right = jnp.concatenate([r for t in blocks for r in plane_rows(wu.at[k], t, cols)], axis=0)
                at = slice(k * 512 + low, k * 512 + low + 256)
                part = jnp.dot(left, right, preferred_element_type=F32)
                up_acc[:, at] = part if first else up_acc[:, at] + part

    def activate():
        r = lax.rsqrt(value["sum"] / (N_TP * width) + EPSILON)
        up = jnp.maximum(up_acc[...] * r * up_scale_ref[...], 0.0)
        hidden[...] = (up * up).astype(BF16)

    def split_middle():
        natural = lax.broadcasted_iota(jnp.int32, (width, width), 0)
        split = lax.broadcasted_iota(jnp.int32, (width, width), 1)
        value["order"] = (
            natural == ((split % 128) // 16) * 32 + (split // 128) * 16 + split % 16
        ).astype(F32).astype(BF16)
        value["split"] = jnp.dot(value["middle"], value["order"], preferred_element_type=F32)

    def down_half(ref):
        def pair(k, blocks):
            pieces = [r for zz in blocks for r in plane_rows(ref.at[k], zz, slice(0, 512))]
            return nt_dot(hidden[:, k * 512:(k + 1) * 512], jnp.concatenate(pieces, axis=0))

        def blocks_of(k, dx):
            blocks = [tp_of(dx, other) for other in (True, False)]
            both = pair(0, blocks) + pair(1, blocks)
            return both[:, 0:128], both[:, 128:256]

        return blocks_of

    def half_out(scatter, cols):
        rounded = (value["split"][:, cols] + scatter.finish()).astype(BF16)
        return nt_dot(rounded, value["order"][:, cols])

    def first_out():
        value["out"] = half_out(scatter2, slice(0, 128))

    def second_out():
        out_ref[...] = (value["out"] + half_out(scatter3, slice(128, 256))).astype(BF16)

    def late_fetches():
        for i in (1, 4, 5, 6, 7, 8, 11, 13):
            fetches[i].wait()

    first_send(D0, 0)
    first_send(D1, 0)
    small_send(SP)
    small_send(SC)
    gather1.begin()
    first_send(U, 0)
    first_forward(D1, 1)
    second_send(D1a)
    first_forward(D0, 1)
    second_send(D0a)
    small_wait(SC, 0)
    small_wait(SP, 0)
    second_send(SPa)
    small_wait(SP, 1)
    gather1.pass_on()
    second_send(SCa)
    second_send(SPb)
    first_forward(U, 1)
    small_wait(SC, 1)
    gather1.near()
    second_send(SCb)
    second_send(Ua)
    first_forward(D1, 2)
    gather1.far()
    forward(SPa, 1)
    first_forward(U, 2)
    forward(SPb, 1)
    gather1.wait(0, 1, 2, 3)
    forward(SCa, 1)
    forward(SCb, 1)
    forward(D0a, 1)
    first_forward(D0, 2)
    late_fetches()
    normalize()
    forward(SPa, 2)
    forward(SPb, 2)
    forward(Ua, 1)
    first_forward(U, 3)
    first_forward(D1, 3)
    first_forward(D0, 3)
    forward(D1a, 1)
    forward(SCa, 2)
    forward(SCb, 2)
    first_wait(U)
    forward(SPa, 3)
    forward(SPb, 3)
    second_send(Ub)
    first_wait(D1)
    forward(SCa, 3)
    forward(SCb, 3)
    second_wait(SPa)
    second_wait(SPb)
    forward(Ua, 2)
    forward(D1a, 2)
    spatial_branch()
    second_send(D1b)
    first_wait(D0)
    second_wait(SCa)
    second_wait(SCb)
    content_branch()
    forward(Ub, 1)
    square_wait()
    second_send(D0b)
    mix()
    forward(D0a, 2)
    scatter1.begin(project_blocks)
    forward(D1b, 1)
    forward(Ub, 2)
    scatter1.combine()
    forward(D0b, 1)
    middle()
    forward(Ua, 3)
    forward(D1b, 2)
    forward(Ub, 3)
    split_middle()
    gather2.wait(0)
    gather2.pass_on()
    gather2.near()
    forward(D0b, 2)
    forward(D1b, 3)
    forward(D1a, 3)
    gather2.wait(1, 2)
    gather2.far()
    second_wait(Ua)
    second_wait(Ub)
    forward(D0a, 3)
    up_part((0,), True)
    up_part((-1, 1))
    gather2.wait(3)
    forward(D0b, 3)
    up_part((2,))
    second_wait(D1b)
    activate()
    second_wait(D1a)
    scatter3.begin(down_half(wd1))
    second_wait(D0b)
    second_wait(D0a)
    scatter2.begin(down_half(wd0))
    scatter3.combine()
    scatter2.combine()
    first_out()
    second_out()
    for u in range(5):
        ref = units[u].at[0, 0:7] if u <= SC else units[u].at[:, 0, 0:7]
        remote(ref, ref, w1_send.at[u], w1_recv.at[u, 0], fs, tp_of(1, False)).wait_send()
    for g in range(10):
        ref = group(g, pl.ds(0, 7))
        remote(ref, ref, w2_send.at[g], w2_recv.at[g, 0], fs, tp_of(1, False)).wait_send()
    gather1.drain()
    gather2.drain()
    scatter1.drain()
    scatter2.drain()
    scatter3.drain()
    remote(squares.at[0:7], squares.at[0:7], sq_send.at[0], sq_recv.at[0], fs, tp_of(1, False)).wait_send()


def shards(
    tokens, mixer_gain, w_content, w_spatial, content_scale, spatial_scale, spatial_gain, block_mixing,
    block_bias, w_project, project_scale, channel_gain, w_up, up_scale, w_down, down_scale,
):
    rows, width = tokens.shape
    row = lambda v: v.reshape(1, -1)
    inputs = (
        tokens, row(mixer_gain), w_content, w_spatial, row(content_scale), row(spatial_scale),
        row(spatial_gain), block_mixing, block_bias, w_project.T, row(project_scale), row(channel_gain),
        w_up, row(up_scale), w_down.T, row(down_scale),
    )
    vmem = pltpu.VMEM
    dma = pltpu.SemaphoreType.DMA
    anywhere = pl.BlockSpec(memory_space=pl.ANY)
    return pl.pallas_call(
        layer_kernel,
        out_shape=pltpu.VMEM((rows, width), BF16),
        in_specs=[anywhere] * N_INPUTS,
        out_specs=pl.BlockSpec(memory_space=pltpu.VMEM),
        scratch_shapes=[vmem(v.shape, v.dtype) for v in inputs] + [
            vmem((RING, RING, SLICE, 128), BF16),
            vmem((RING, RING, SLICE, 256), BF16),
            vmem((2, RING, RING, SLICE, 512), BF16),
            vmem((2, RING, RING, SLICE // 2, 512), BF16),
            vmem((2, RING, RING, SLICE // 2, 512), BF16),
            vmem((N_TP, rows, width), BF16),
            vmem((N_TP, rows, width), BF16),
            vmem((rows, N_TP * width), BF16),
            vmem((N_TP, 8, rows), F32),
            vmem((rows, w_up.shape[1]), BF16),
            vmem((rows, w_up.shape[1]), F32),
            vmem((4, rows, 256), BF16), vmem((4, rows, 256), BF16), vmem((3, rows, 256), BF16),
            vmem((2, rows // 2, 256), BF16), vmem((2, rows, 256), BF16), vmem((4, rows, 256), F32),
            vmem((8, rows, 128), BF16), vmem((8, rows, 128), BF16), vmem((6, rows, 128), BF16),
            vmem((4, rows // 2, 128), BF16), vmem((4, rows, 128), BF16), vmem((8, rows, 128), F32),
            dma((N_INPUTS,)), dma((5,)), dma((5, HOPS)), dma((10,)), dma((10, HOPS)),
            dma((2,)), dma((2, 10)), dma((3,)), dma((3, 10)), dma((1,)), dma((7,)),
        ],
        compiler_params=pltpu.CompilerParams(
            collective_id=0, has_side_effects=True, vmem_limit_bytes=56 * 1024 * 1024),
        name="layer",
    )(*inputs)


def solution(mesh):
    return jax.shard_map(
        shards,
        mesh=mesh,
        in_specs=(
            P("fs", "tp"), P(), P("fs", "tp"), P("fs", "tp"), P("tp"), P("tp"), P("tp"),
            P("tp", None, None), P("tp", None), P("tp", "fs"), P("fs"), P(), P("fs", "tp"), P("tp"),
            P("tp", "fs"), P("fs"),
        ),
        out_specs=P("fs", "tp"),
        check_vma=False,
    )
```

```python
import jax
import jax.numpy as jnp
from jax import lax
from jax.experimental import pallas as pl
from jax.experimental.pallas import tpu as pltpu
from jax.sharding import PartitionSpec as P

EPSILON = 1e-06
MESH = pl.DeviceIdType.MESH
F32 = jnp.float32
BF16 = jnp.bfloat16

RING = 8
HOPS = RING // 2
CHIPS_X = 4
N_TP = 2 * CHIPS_X
SLICE = 32
BLOCK = 128
N_INPUTS = 16


def nt_dot(left, right):
    return lax.dot_general(left, right, (((1,), (1,)), ((), ())), preferred_element_type=F32)


def layer_kernel(*refs):
    hbm = refs[:N_INPUTS]
    out_ref = refs[N_INPUTS]
    inputs = refs[N_INPUTS + 1:2 * N_INPUTS + 1]
    (
        tokens_ref, mixer_gain_ref, w_content_ref, w_spatial_ref, content_scale_ref, spatial_scale_ref,
        spatial_gain_ref, mixing_ref, bias_ref, w_project_ref, project_scale_ref, channel_gain_ref,
        w_up_ref, up_scale_ref, w_down_ref, down_scale_ref,
    ) = inputs
    (
        wp, wc, wu, wd0, wd1, tok1, tok2, normed, squares, hidden, up_acc,
        sib_out1, sib_in1, ring_out1, far_in1, near_in1, acc1,
        sib_out2, sib_in2, ring_out2, far_in2, near_in2, acc2,
        in_sem, w1_send, w1_recv, w2_send, w2_recv,
        ag_send, ag_recv, rs_send, rs_recv, sq_send, sq_recv,
    ) = refs[2 * N_INPUTS + 1:]
    fs, tp = lax.axis_index("fs"), lax.axis_index("tp")
    z, y = fs // RING, fs % RING
    x, core = tp // 2, tp % 2
    p = jnp.where(core == 0, y, z)
    q = jnp.where(core == 0, z, y)

    def fs_of(pp, qq):
        return jnp.where(core == 0, qq * RING + pp, pp * RING + qq)

    def tp_of(dx, other):
        c = (1 - core) if other else core
        return 2 * ((x + dx + CHIPS_X) % CHIPS_X) + c

    first_next = (fs_of((p + 1) % RING, q), fs_of((p + RING - 1) % RING, q))
    second_next = (fs_of(p, (q + 1) % RING), fs_of(p, (q + RING - 1) % RING))

    barrier = pltpu.get_barrier_semaphore()
    for to in tuple(fs_of((p + d) % RING, q) for d in range(1, RING)) + second_next:
        pl.semaphore_signal(barrier, inc=1, device_id=(to, tp), device_id_type=MESH)
    for d in range(1, N_TP):
        pl.semaphore_signal(barrier, inc=1, device_id=(fs, (tp + d) % N_TP), device_id_type=MESH)
    fetches = [pltpu.make_async_copy(hbm[i], inputs[i], in_sem.at[i]) for i in range(N_INPUTS)]
    for i in (2, 3, 9, 10, 0, 12, 14, 15, 1, 4, 5, 6, 7, 8, 11, 13):
        fetches[i].start()

    def remote(src, dst, ss, rs, to_fs, to_tp):
        return pltpu.make_async_remote_copy(
            src_ref=src, dst_ref=dst, send_sem=ss, recv_sem=rs,
            device_id=(to_fs, to_tp), device_id_type=MESH,
        )

    eye = (
        lax.broadcasted_iota(jnp.int32, (SLICE, SLICE), 0)
        == lax.broadcasted_iota(jnp.int32, (SLICE, SLICE), 1)
    )

    def scaled(w, scale):
        column = jnp.sum(jnp.where(eye, scale, 0.0), axis=1, keepdims=True)
        return (w.astype(BF16).astype(F32) * column).astype(BF16)

    for i in (2, 3, 9, 10):
        fetches[i].wait()
    wp[q, 0] = w_spatial_ref[...].astype(BF16)
    wc[q, 0, :, 0:128] = w_content_ref[...].astype(BF16)
    wc[q, 0, :, 128:256] = scaled(w_project_ref[...], project_scale_ref[...])
    for i in (0, 12, 14, 15):
        fetches[i].wait()
    tok1[tp] = tokens_ref[...]
    down = scaled(w_down_ref[...], down_scale_ref[...])
    for k in range(2):
        cols = slice(k * 512, (k + 1) * 512)
        wu[k, q, 0] = w_up_ref[:, cols].astype(BF16)
        wd0[k, q, 0] = down[0:16, cols]
        wd1[k, q, 0] = down[16:32, cols]
    pl.semaphore_wait(barrier, RING - 1 + 2 + N_TP - 1)

    SP, SC, U, D0, D1 = range(5)
    units = (wp, wc, wu, wd0, wd1)

    def first_copy(u, src, dst, to, sem, part=None):
        if u <= SC:
            src_ref, dst_ref = units[u].at[q, src], units[u].at[q, dst]
        else:
            lead = slice(None) if part is None else part
            src_ref, dst_ref = units[u].at[lead, q, src], units[u].at[lead, q, dst]
        return remote(src_ref, dst_ref, w1_send.at[u], w1_recv.at[u, sem], to, tp)

    places = {0: 0, 1: 1, -1: 2, 2: 3, -2: 4, 3: 5, -3: 6, 4: 7, -4: 7}

    def first_send(u, step):
        for way in range(2):
            sign = 1 if way else -1
            first_copy(u, places[sign * step], places[sign * (step + 1)], first_next[way], step,
                       way if step == HOPS - 1 else None).start()

    def small_send(u):
        for d in (1, -1, 2, -2, 3, -3, 4):
            first_copy(u, 0, places[-d], fs_of((p + d + RING) % RING, q), 0 if abs(d) == 1 else 1).start()

    def small_wait(u, sem):
        ref = units[u].at[0, 0:2] if sem == 0 else units[u].at[0, 0:5]
        remote(ref, ref, w1_send.at[u], w1_recv.at[u, sem], first_next[0], tp).wait_recv()

    def first_wait(u, distance=HOPS):
        n = 1 if distance == HOPS else 2
        ref = units[u].at[:, 0, 0:n]
        remote(ref, ref, w1_send.at[u], w1_recv.at[u, distance - 1], first_next[0], tp).wait_recv()

    def first_forward(u, step):
        first_wait(u, step)
        first_send(u, step)

    SPa, SPb, SCa, SCb, Uo, Ua, Ub, D0o, D0a, D0b, D1o, D1a, D1b = range(13)
    SMALL = 4
    groups = [(u, low, n) for u in (SP, SC) for low, n in ((0, 3), (3, 5))]
    groups += [(u, low, n) for u in (U, D0, D1) for low, n in ((0, 1), (1, 2), (3, 5))]

    def group(g, at, lead=slice(None)):
        u, low, n = groups[g]
        shards_of = pl.ds(low, n)
        return units[u].at[at, shards_of] if g < SMALL else units[u].at[lead, at, shards_of]

    def second_copy(g, way, step):
        at = (q + (step if way else -step) + RING) % RING
        ref = group(g, at)
        if step == HOPS - 1:
            ref = ref.at[:, pl.ds(way * (SLICE // 2), SLICE // 2)] if g < SMALL else group(g, at, way)
        return remote(ref, ref, w2_send.at[g], w2_recv.at[g, step], second_next[way], tp)

    def second_send(g, step=0):
        for way in range(2):
            second_copy(g, way, step).start()

    def second_wait(g, step=HOPS - 1):
        ref = group(g, 0) if step == HOPS - 1 else group(g, pl.ds(0, 2))
        remote(ref, ref, w2_send.at[g], w2_recv.at[g, step], second_next[0], tp).wait_recv()

    def forward(g, step):
        second_wait(g, step - 1)
        second_send(g, step)

    half = tokens_ref.shape[0] // 2

    class Gather:
        def __init__(self, buf, n):
            self.buf, self.n = buf, n

        def copy(self, k, arriving=False):
            dx = (0, -1, 1, 2, 0, 0, 0, 0, -1, 1)[k]
            if arriving and k >= 4:
                dx = (-1, 1, -1, 1, -2, 2)[k - 4]
            ref = self.buf.at[tp_of(dx, arriving and k < 4)]
            if k >= 4:
                ref = ref.at[pl.ds((k % 2 if k // 2 != 3 else 1 - k % 2) * half, half)]
            to = tp_of(0, True) if k < 4 else tp_of((1, -1)[k % 2], False)
            return remote(ref, ref, ag_send.at[self.n], ag_recv.at[self.n, k], fs, to)

        def begin(self):
            for k in (4, 5, 6, 7, 0):
                self.copy(k).start()

        def pass_on(self):
            for k in range(2):
                self.copy(4 + k, True).wait_recv()
                self.copy(8 + k).start()

        def near(self):
            for k in range(2):
                self.copy(6 + k, True).wait_recv()
                self.copy(1 + k).start()

        def far(self):
            for k in range(2):
                self.copy(8 + k, True).wait_recv()
            self.copy(3).start()

        def wait(self, *which):
            for k in which:
                self.copy(k, True).wait_recv()

        def drain(self):
            ref = self.buf.at[0:7]
            remote(ref, ref, ag_send.at[self.n], ag_recv.at[self.n, 0], fs, tp_of(1, False)).wait_send()

    class Scatter:
        order = (2, 1, -1, 0)

        def __init__(self, n, bufs, bytes_ref):
            self.n, self.bytes_ref = n, bytes_ref
            self.sib_out, self.sib_in, self.ring_out, self.far_in, self.near_in, self.acc = bufs

        def copy(self, src, dst, k, to):
            return remote(src, dst, rs_send.at[self.n], rs_recv.at[self.n, k], fs, to)

        def across(self, k):
            return self.copy(self.sib_out.at[k], self.sib_in.at[k], k, tp_of(0, True))

        def far(self, way):
            return self.copy(self.ring_out.at[0, pl.ds(way * half, half)], self.far_in.at[way], 4 + way,
                             tp_of((1, -1)[way], False))

        def near(self, way, part):
            rows = pl.ds(part * half, half)
            return self.copy(self.ring_out.at[1 + way, rows], self.near_in.at[way, rows], 6,
                             tp_of((1, -1)[way], False))

        def begin(self, blocks_of):
            for k, dx in enumerate(self.order):
                across, own = blocks_of(k, dx)
                self.sib_out[k] = across.astype(BF16)
                self.across(k).start()
                self.acc[k] = own
                if k > 1:
                    self.own(k - 2)
            self.own(2)

        def own(self, k):
            self.across(k).wait_recv()
            value = self.acc[k] + self.sib_in[k].astype(F32)
            if k == 0:
                self.ring_out[0] = value.astype(BF16)
                self.far(0).start()
                self.far(1).start()
            else:
                self.acc[k] = value
                if k < 3:
                    part = 2 - k
                    rows = slice(part * half, (part + 1) * half)
                    self.ring_out[k, rows] = value[rows].astype(BF16)
                    self.near(k - 1, part).start()

        def combine(self):
            for way in range(2):
                self.far(way).wait_recv()
                rows = slice(way * half, (way + 1) * half)
                self.ring_out[1 + way, rows] = (
                    self.acc[1 + way, rows] + self.far_in[way].astype(F32)).astype(BF16)
                self.near(way, way).start()

        def finish(self):
            self.own(3)
            self.copy(self.near_in, self.near_in, 6, tp_of(1, False)).wait_recv()
            return self.acc[3] + self.near_in[0].astype(F32) + self.near_in[1].astype(F32)

        def drain(self):
            remote(self.bytes_ref, self.bytes_ref, rs_send.at[self.n], rs_recv.at[self.n, 0], fs,
                   tp_of(1, False)).wait_send()

    width = tokens_ref.shape[1]

    def normalize():
        total = None
        for t in range(N_TP):
            v = tok1[t].astype(F32)
            s = jnp.sum(v * v, axis=1, keepdims=True)
            total = s if total is None else total + s
        r = lax.rsqrt(total / (N_TP * width) + EPSILON)
        for t in range(N_TP):
            cols = slice(t * width, (t + 1) * width)
            normed[:, cols] = (tok1[t].astype(F32) * r * mixer_gain_ref[:, cols]).astype(BF16)

    def plane_rows(ref, zz, cols):
        rows = []
        for j in range(RING):
            first, second = jnp.where(core == 0, j, zz), jnp.where(core == 0, zz, j)
            d = (first - p + RING) % RING
            at = jnp.where((d >= 1) & (d <= HOPS), 2 * d - 1, (2 * (RING - d)) % (2 * RING))
            rows.append(ref[second, at, :, cols])
        return rows

    def all_rows(ref, cols):
        return jnp.concatenate([r for zz in range(RING) for r in plane_rows(ref, zz, cols)], axis=0)

    def set_of(*bufs, low=None):
        return bufs if low is None else tuple(b.at[pl.ds(low * (b.shape[0] // 2), b.shape[0] // 2)] for b in bufs)

    gather1, gather2 = Gather(tok1, 0), Gather(tok2, 1)
    bufs2 = (sib_out2, sib_in2, ring_out2, far_in2, near_in2, acc2)
    scatter1 = Scatter(0, (sib_out1, sib_in1, ring_out1, far_in1, near_in1, acc1), tok1.at[0:7])
    scatter2 = Scatter(1, set_of(*bufs2, low=0), sib_out2.at[0:7])
    scatter3 = Scatter(2, set_of(*bufs2, low=1), sib_out2.at[0:7])

    value = {}

    def square_copy(d):
        ref = squares.at[tp]
        return remote(ref, ref, sq_send.at[0], sq_recv.at[0], fs, (tp + d) % N_TP)

    def spatial_branch():
        linear = jnp.dot(normed[...], all_rows(wp, slice(0, 128)), preferred_element_type=F32)
        spatial = jax.nn.gelu(linear * spatial_scale_ref[...])
        sq = spatial * spatial
        sq_high = sq.astype(BF16)
        sq_low = (sq - sq_high.astype(F32)).astype(BF16)
        ones = jnp.ones((8, 128), BF16)
        squares[tp] = nt_dot(ones, sq_high) + nt_dot(ones, sq_low)
        for d in range(1, N_TP):
            square_copy(d).start()
        value["gained"] = (spatial * spatial_gain_ref[...]).astype(BF16)

    def content_branch():
        linear = jnp.dot(normed[...], all_rows(wc, slice(0, 128)), preferred_element_type=F32)
        value["content"] = jax.nn.gelu(linear * content_scale_ref[...])
        causal = (
            lax.broadcasted_iota(jnp.int32, (BLOCK, BLOCK), 1)
            <= lax.broadcasted_iota(jnp.int32, (BLOCK, BLOCK), 0)
        )
        value["mixing"] = jnp.where(causal, mixing_ref[0].astype(F32), 0.0)
        value["bias"] = jnp.transpose(jnp.broadcast_to(bias_ref[...], (BLOCK, BLOCK)))

    def square_wait():
        ref = squares.at[0:N_TP - 1]
        remote(ref, ref, sq_send.at[0], sq_recv.at[0], fs, tp_of(1, False)).wait_recv()

    def mix():
        total_sq = squares[0]
        for t in range(1, N_TP):
            total_sq = total_sq + squares[t]
        row_scale = lax.rsqrt(total_sq[0:1] / (N_TP * 128) + EPSILON)
        gated = []
        for b in range(tokens_ref.shape[0] // BLOCK):
            rows = slice(b * BLOCK, (b + 1) * BLOCK)
            mixing_b = (value["mixing"] * row_scale[:, rows]).astype(BF16)
            mixed = jnp.dot(mixing_b, value["gained"][rows], preferred_element_type=F32) + value["bias"]
            gated.append((value["content"][rows] * mixed).astype(BF16))
        value["gated"] = jnp.concatenate(gated, axis=0)

    def project_blocks(k, dx):
        return tuple(
            nt_dot(value["gated"], jnp.concatenate(plane_rows(wc, tp_of(dx, other), slice(128, 256)), axis=0))
            for other in (True, False))

    def middle():
        value["middle"] = (tokens_ref[...].astype(F32) + scatter1.finish()).astype(BF16)
        tok2[tp] = value["middle"]
        gather2.begin()

    def up_part(dxs, first=False):
        blocks = [tp_of(dx, other) for dx in dxs for other in (False, True)]
        terms = []
        for t in blocks:
            v = tok2[t].astype(F32)
            s = jnp.sum(v * v, axis=1, keepdims=True)
            value["sum"] = s if first and not terms else value["sum"] + s
            gain = channel_gain_ref[:, pl.ds(pl.multiple_of(t * width, 128), width)]
            terms.append((v * gain).astype(BF16))
        left = jnp.concatenate(terms, axis=1)
        for k in range(2):
            for low in range(0, 512, 256):
                cols = slice(low, low + 256)
                right = jnp.concatenate([r for t in blocks for r in plane_rows(wu.at[k], t, cols)], axis=0)
                at = slice(k * 512 + low, k * 512 + low + 256)
                part = jnp.dot(left, right, preferred_element_type=F32)
                up_acc[:, at] = part if first else up_acc[:, at] + part

    def activate():
        r = lax.rsqrt(value["sum"] / (N_TP * width) + EPSILON)
        up = jnp.maximum(up_acc[...] * r * up_scale_ref[...], 0.0)
        hidden[...] = (up * up).astype(BF16)

    def split_middle():
        natural = lax.broadcasted_iota(jnp.int32, (width, width), 0)
        split = lax.broadcasted_iota(jnp.int32, (width, width), 1)
        value["order"] = (
            natural == ((split % 128) // 16) * 32 + (split // 128) * 16 + split % 16
        ).astype(F32).astype(BF16)
        value["split"] = jnp.dot(value["middle"], value["order"], preferred_element_type=F32)

    def down_half(ref):
        def blocks_of(k, dx):
            rows = [
                jnp.concatenate(halves, axis=1)
                for other in (True, False)
                for halves in zip(*(plane_rows(ref.at[i], tp_of(dx, other), slice(0, 512)) for i in range(2)))
            ]
            both = nt_dot(hidden[...], jnp.concatenate(rows, axis=0))
            return both[:, 0:128], both[:, 128:256]

        return blocks_of

    def half_out(scatter, cols):
        rounded = (value["split"][:, cols] + scatter.finish()).astype(BF16)
        return nt_dot(rounded, value["order"][:, cols])

    def first_out():
        value["out"] = half_out(scatter2, slice(0, 128))

    def second_out():
        out_ref[...] = (value["out"] + half_out(scatter3, slice(128, 256))).astype(BF16)

    def late_fetches():
        for i in (1, 4, 5, 6, 7, 8, 11, 13):
            fetches[i].wait()

    first_send(D1, 0)
    gather1.begin()
    first_send(U, 0)
    small_send(SP)
    first_send(D0, 0)
    small_send(SC)
    first_forward(D1, 1)
    second_send(D0o)
    first_forward(U, 1)
    small_wait(SP, 0)
    second_send(SPa)
    second_send(Ua)
    small_wait(SC, 0)
    second_send(D1o)
    gather1.pass_on()
    second_send(SCa)
    small_wait(SP, 1)
    second_send(SPb)
    first_forward(D0, 1)
    second_send(D1a)
    forward(SPa, 1)
    small_wait(SC, 1)
    second_send(SCb)
    first_forward(U, 2)
    forward(Ua, 1)
    forward(SPb, 1)
    first_forward(D1, 2)
    forward(SCa, 1)
    forward(D1o, 1)
    second_send(Uo)
    gather1.far()
    gather1.near()
    forward(SPa, 2)
    forward(SCb, 1)
    gather1.wait(0, 1, 2, 3)
    first_forward(U, 3)
    first_forward(D0, 2)
    forward(D1a, 1)
    forward(SPb, 2)
    forward(SCa, 2)
    second_send(D0a)
    forward(Ua, 2)
    forward(SCb, 2)
    first_forward(D1, 3)
    first_wait(U)
    forward(SPa, 3)
    first_forward(D0, 3)
    forward(SPb, 3)
    forward(D0o, 1)
    forward(SCa, 3)
    second_send(Ub)
    late_fetches()
    normalize()
    second_wait(SPb)
    forward(SCb, 3)
    first_wait(D1)
    forward(Uo, 1)
    second_send(D1b)
    forward(Ua, 3)
    second_wait(SPa)
    spatial_branch()
    forward(D0o, 2)
    forward(Ub, 1)
    first_wait(D0)
    second_wait(SCa)
    second_send(D0b)
    second_wait(SCb)
    content_branch()
    forward(D0a, 1)
    forward(D1a, 2)
    square_wait()
    mix()
    scatter1.begin(project_blocks)
    forward(Uo, 2)
    forward(D1b, 1)
    forward(Ub, 2)
    scatter1.combine()
    forward(D0b, 1)
    second_wait(Ua)
    forward(D1o, 2)
    middle()
    forward(Uo, 3)
    forward(D1b, 2)
    forward(Ub, 3)
    forward(D0a, 2)
    gather2.pass_on()
    forward(D0b, 2)
    forward(D1o, 3)
    gather2.near()
    forward(D1b, 3)
    second_wait(Uo)
    forward(D1a, 3)
    gather2.wait(0)
    second_wait(Ub)
    up_part((0,), True)
    gather2.far()
    split_middle()
    forward(D0o, 3)
    forward(D0a, 3)
    gather2.wait(1, 2)
    up_part((-1, 1))
    gather2.wait(3)
    forward(D0b, 3)
    second_wait(D1o)
    up_part((2,))
    second_wait(D1b)
    activate()
    second_wait(D1a)
    scatter3.begin(down_half(wd1))
    second_wait(D0a)
    second_wait(D0o)
    second_wait(D0b)
    scatter2.begin(down_half(wd0))
    scatter3.combine()
    scatter2.combine()
    first_out()
    second_out()
    for u in range(5):
        ref = units[u].at[0, 0:7] if u <= SC else units[u].at[:, 0, 0:7]
        remote(ref, ref, w1_send.at[u], w1_recv.at[u, 0], fs, tp_of(1, False)).wait_send()
    for g in range(13):
        ref = group(g, pl.ds(0, 7))
        remote(ref, ref, w2_send.at[g], w2_recv.at[g, 0], fs, tp_of(1, False)).wait_send()
    gather1.drain()
    gather2.drain()
    scatter1.drain()
    scatter2.drain()
    scatter3.drain()
    remote(squares.at[0:7], squares.at[0:7], sq_send.at[0], sq_recv.at[0], fs, tp_of(1, False)).wait_send()


def shards(
    tokens, mixer_gain, w_content, w_spatial, content_scale, spatial_scale, spatial_gain, block_mixing,
    block_bias, w_project, project_scale, channel_gain, w_up, up_scale, w_down, down_scale,
):
    rows, width = tokens.shape
    row = lambda v: v.reshape(1, -1)
    inputs = (
        tokens, row(mixer_gain), w_content, w_spatial, row(content_scale), row(spatial_scale),
        row(spatial_gain), block_mixing, block_bias, w_project.T, row(project_scale), row(channel_gain),
        w_up, row(up_scale), w_down.T, row(down_scale),
    )
    vmem = pltpu.VMEM
    dma = pltpu.SemaphoreType.DMA
    anywhere = pl.BlockSpec(memory_space=pl.ANY)
    return pl.pallas_call(
        layer_kernel,
        out_shape=pltpu.VMEM((rows, width), BF16),
        in_specs=[anywhere] * N_INPUTS,
        out_specs=pl.BlockSpec(memory_space=pltpu.VMEM),
        scratch_shapes=[vmem(v.shape, v.dtype) for v in inputs] + [
            vmem((RING, RING, SLICE, 128), BF16),
            vmem((RING, RING, SLICE, 256), BF16),
            vmem((2, RING, RING, SLICE, 512), BF16),
            vmem((2, RING, RING, SLICE // 2, 512), BF16),
            vmem((2, RING, RING, SLICE // 2, 512), BF16),
            vmem((N_TP, rows, width), BF16),
            vmem((N_TP, rows, width), BF16),
            vmem((rows, N_TP * width), BF16),
            vmem((N_TP, 8, rows), F32),
            vmem((rows, w_up.shape[1]), BF16),
            vmem((rows, w_up.shape[1]), F32),
            vmem((4, rows, 256), BF16), vmem((4, rows, 256), BF16), vmem((3, rows, 256), BF16),
            vmem((2, rows // 2, 256), BF16), vmem((2, rows, 256), BF16), vmem((4, rows, 256), F32),
            vmem((8, rows, 128), BF16), vmem((8, rows, 128), BF16), vmem((6, rows, 128), BF16),
            vmem((4, rows // 2, 128), BF16), vmem((4, rows, 128), BF16), vmem((8, rows, 128), F32),
            dma((N_INPUTS,)), dma((5,)), dma((5, HOPS)), dma((13,)), dma((13, HOPS)),
            dma((2,)), dma((2, 10)), dma((3,)), dma((3, 7)), dma((1,)), dma((1,)),
        ],
        compiler_params=pltpu.CompilerParams(
            collective_id=0, has_side_effects=True, vmem_limit_bytes=56 * 1024 * 1024),
        name="layer",
    )(*inputs)


def solution(mesh):
    return jax.shard_map(
        shards,
        mesh=mesh,
        in_specs=(
            P("fs", "tp"), P(), P("fs", "tp"), P("fs", "tp"), P("tp"), P("tp"), P("tp"),
            P("tp", None, None), P("tp", None), P("tp", "fs"), P("fs"), P(), P("fs", "tp"), P("tp"),
            P("tp", "fs"), P("fs"),
        ),
        out_specs=P("fs", "tp"),
        check_vma=False,
    )
```

```python
import jax
import jax.numpy as jnp
from jax import lax
from jax.experimental import pallas as pl
from jax.experimental.pallas import tpu as pltpu
from jax.sharding import PartitionSpec as P

EPSILON = 1e-06
MESH = pl.DeviceIdType.MESH
F32 = jnp.float32
BF16 = jnp.bfloat16

RING = 8
HOPS = RING // 2
CHIPS_X = 4
N_TP = 2 * CHIPS_X
SLICE = 32
BLOCK = 128
N_INPUTS = 16


def nt_dot(left, right):
    return lax.dot_general(left, right, (((1,), (1,)), ((), ())), preferred_element_type=F32)


def layer_kernel(*refs):
    hbm = refs[:N_INPUTS]
    out_ref = refs[N_INPUTS]
    inputs = refs[N_INPUTS + 1:2 * N_INPUTS + 1]
    (
        tokens_ref, mixer_gain_ref, w_content_ref, w_spatial_ref, content_scale_ref, spatial_scale_ref,
        spatial_gain_ref, mixing_ref, bias_ref, w_project_ref, project_scale_ref, channel_gain_ref,
        w_up_ref, up_scale_ref, w_down_ref, down_scale_ref,
    ) = inputs
    (
        wp, wc, wu, wd0, wd1, tok1, tok2, normed, squares, hidden, up_acc,
        sib_out1, sib_in1, ring_out1, far_in1, near_in1, acc1,
        sib_out2, sib_in2, ring_out2, far_in2, near_in2, acc2,
        in_sem, w1_send, w1_recv, w2_send, w2_recv,
        ag_send, ag_recv, rs_send, rs_recv, sq_send, sq_recv,
    ) = refs[2 * N_INPUTS + 1:]
    fs, tp = lax.axis_index("fs"), lax.axis_index("tp")
    z, y = fs // RING, fs % RING
    x, core = tp // 2, tp % 2
    p = jnp.where(core == 0, y, z)
    q = jnp.where(core == 0, z, y)

    def fs_of(pp, qq):
        return jnp.where(core == 0, qq * RING + pp, pp * RING + qq)

    def tp_of(dx, other):
        c = (1 - core) if other else core
        return 2 * ((x + dx + CHIPS_X) % CHIPS_X) + c

    first_next = (fs_of((p + 1) % RING, q), fs_of((p + RING - 1) % RING, q))
    second_next = (fs_of(p, (q + 1) % RING), fs_of(p, (q + RING - 1) % RING))

    barrier = pltpu.get_barrier_semaphore()
    for to in tuple(fs_of(p, (q + d) % RING) for d in range(1, RING)) + first_next:
        pl.semaphore_signal(barrier, inc=1, device_id=(to, tp), device_id_type=MESH)
    for d in range(1, N_TP):
        pl.semaphore_signal(barrier, inc=1, device_id=(fs, (tp + d) % N_TP), device_id_type=MESH)
    fetches = [pltpu.make_async_copy(hbm[i], inputs[i], in_sem.at[i]) for i in range(N_INPUTS)]
    for i in (2, 3, 9, 10, 0, 12, 14, 15, 1, 4, 5, 6, 7, 8, 11, 13):
        fetches[i].start()

    def remote(src, dst, ss, rs, to_fs, to_tp):
        return pltpu.make_async_remote_copy(
            src_ref=src, dst_ref=dst, send_sem=ss, recv_sem=rs,
            device_id=(to_fs, to_tp), device_id_type=MESH,
        )

    eye = (
        lax.broadcasted_iota(jnp.int32, (SLICE, SLICE), 0)
        == lax.broadcasted_iota(jnp.int32, (SLICE, SLICE), 1)
    )

    def scaled(w, scale):
        column = jnp.sum(jnp.where(eye, scale, 0.0), axis=1, keepdims=True)
        return (w.astype(BF16).astype(F32) * column).astype(BF16)

    for i in (2, 3, 9, 10):
        fetches[i].wait()
    wp[p, 0] = w_spatial_ref[...].astype(BF16)
    wc[p, 0, :, 0:128] = w_content_ref[...].astype(BF16)
    wc[p, 0, :, 128:256] = scaled(w_project_ref[...], project_scale_ref[...])
    for i in (0, 12, 14, 15):
        fetches[i].wait()
    tok1[tp] = tokens_ref[...]
    down = scaled(w_down_ref[...], down_scale_ref[...])
    for k in range(2):
        cols = slice(k * 512, (k + 1) * 512)
        wu[k, q, 0] = w_up_ref[:, cols].astype(BF16)
        wd0[k, q, 0] = down[0:16, cols]
        wd1[k, q, 0] = down[16:32, cols]
    pl.semaphore_wait(barrier, RING - 1 + 2 + N_TP - 1)

    SP, SC, U, D0, D1 = range(5)
    units = (wp, wc, wu, wd0, wd1)

    def first_copy(u, src, dst, to, sem, part=None):
        if u <= SC:
            src_ref, dst_ref = units[u].at[p, src], units[u].at[p, dst]
        else:
            lead = slice(None) if part is None else part
            src_ref, dst_ref = units[u].at[lead, q, src], units[u].at[lead, q, dst]
        return remote(src_ref, dst_ref, w1_send.at[u], w1_recv.at[u, sem], to, tp)

    places = {0: 0, 1: 1, -1: 2, 2: 3, -2: 4, 3: 5, -3: 6, 4: 7, -4: 7}

    def first_send(u, step):
        for way in range(2):
            sign = 1 if way else -1
            first_copy(u, places[sign * step], places[sign * (step + 1)], first_next[way], step,
                       way if step == HOPS - 1 else None).start()

    def small_send(u):
        for d in (1, -1, 2, -2, 3, -3, 4):
            first_copy(u, 0, places[-d], fs_of(p, (q + d + RING) % RING), 0 if abs(d) == 1 else 1).start()

    def small_wait(u, sem):
        ref = units[u].at[0, 0:2] if sem == 0 else units[u].at[0, 0:5]
        remote(ref, ref, w1_send.at[u], w1_recv.at[u, sem], first_next[0], tp).wait_recv()

    def first_wait(u, distance=HOPS):
        n = 1 if distance == HOPS else 2
        ref = units[u].at[:, 0, 0:n]
        remote(ref, ref, w1_send.at[u], w1_recv.at[u, distance - 1], first_next[0], tp).wait_recv()

    def first_forward(u, step):
        first_wait(u, step)
        first_send(u, step)

    SPa, SPb, SCa, SCb, Uo, Ua, Ub, D0o, D0a, D0b, D1o, D1a, D1b = range(13)
    SMALL = 4
    groups = [(u, low, n) for u in (SP, SC) for low, n in ((0, 3), (3, 5))]
    groups += [(u, low, n) for u in (U, D0, D1) for low, n in ((0, 1), (1, 2), (3, 5))]

    def group(g, at, lead=slice(None)):
        u, low, n = groups[g]
        shards_of = pl.ds(low, n)
        return units[u].at[at, shards_of] if g < SMALL else units[u].at[lead, at, shards_of]

    def second_copy(g, way, step):
        start, to = (p, first_next) if g < SMALL else (q, second_next)
        at = (start + (step if way else -step) + RING) % RING
        ref = group(g, at)
        if step == HOPS - 1:
            ref = ref.at[:, pl.ds(way * (SLICE // 2), SLICE // 2)] if g < SMALL else group(g, at, way)
        return remote(ref, ref, w2_send.at[g], w2_recv.at[g, step], to[way], tp)

    def second_send(g, step=0):
        for way in range(2):
            second_copy(g, way, step).start()

    def second_wait(g, step=HOPS - 1):
        ref = group(g, 0) if step == HOPS - 1 else group(g, pl.ds(0, 2))
        remote(ref, ref, w2_send.at[g], w2_recv.at[g, step], second_next[0], tp).wait_recv()

    def forward(g, step):
        second_wait(g, step - 1)
        second_send(g, step)

    half = tokens_ref.shape[0] // 2

    class Gather:
        def __init__(self, buf, n):
            self.buf, self.n = buf, n

        def copy(self, k, arriving=False):
            dx = (0, -1, 1, 2, 0, 0, 0, 0, -1, 1)[k]
            if arriving and k >= 4:
                dx = (-1, 1, -1, 1, -2, 2)[k - 4]
            ref = self.buf.at[tp_of(dx, arriving and k < 4)]
            if k >= 4:
                ref = ref.at[pl.ds((k % 2 if k // 2 != 3 else 1 - k % 2) * half, half)]
            to = tp_of(0, True) if k < 4 else tp_of((1, -1)[k % 2], False)
            return remote(ref, ref, ag_send.at[self.n], ag_recv.at[self.n, k], fs, to)

        def begin(self):
            for k in (4, 5, 6, 7, 0):
                self.copy(k).start()

        def pass_on(self):
            for k in range(2):
                self.copy(4 + k, True).wait_recv()
                self.copy(8 + k).start()

        def near(self):
            for k in range(2):
                self.copy(6 + k, True).wait_recv()
                self.copy(1 + k).start()

        def far(self):
            for k in range(2):
                self.copy(8 + k, True).wait_recv()
            self.copy(3).start()

        def wait(self, *which):
            for k in which:
                self.copy(k, True).wait_recv()

        def drain(self):
            ref = self.buf.at[0:7]
            remote(ref, ref, ag_send.at[self.n], ag_recv.at[self.n, 0], fs, tp_of(1, False)).wait_send()

    class Scatter:
        order = (2, 1, -1, 0)

        def __init__(self, n, bufs, bytes_ref):
            self.n, self.bytes_ref = n, bytes_ref
            self.sib_out, self.sib_in, self.ring_out, self.far_in, self.near_in, self.acc = bufs

        def copy(self, src, dst, k, to):
            return remote(src, dst, rs_send.at[self.n], rs_recv.at[self.n, k], fs, to)

        def across(self, k):
            return self.copy(self.sib_out.at[k], self.sib_in.at[k], k, tp_of(0, True))

        def far(self, way):
            return self.copy(self.ring_out.at[0, pl.ds(way * half, half)], self.far_in.at[way], 4 + way,
                             tp_of((1, -1)[way], False))

        def near(self, way, part):
            rows = pl.ds(part * half, half)
            return self.copy(self.ring_out.at[1 + way, rows], self.near_in.at[way, rows], 6,
                             tp_of((1, -1)[way], False))

        def begin(self, blocks_of):
            for k, dx in enumerate(self.order):
                across, own = blocks_of(k, dx)
                self.sib_out[k] = across.astype(BF16)
                self.across(k).start()
                self.acc[k] = own
                if k > 1:
                    self.own(k - 2)
            self.own(2)

        def own(self, k):
            self.across(k).wait_recv()
            value = self.acc[k] + self.sib_in[k].astype(F32)
            if k == 0:
                self.ring_out[0] = value.astype(BF16)
                self.far(0).start()
                self.far(1).start()
            else:
                self.acc[k] = value
                if k < 3:
                    part = 2 - k
                    rows = slice(part * half, (part + 1) * half)
                    self.ring_out[k, rows] = value[rows].astype(BF16)
                    self.near(k - 1, part).start()

        def combine(self):
            for way in range(2):
                self.far(way).wait_recv()
                rows = slice(way * half, (way + 1) * half)
                self.ring_out[1 + way, rows] = (
                    self.acc[1 + way, rows] + self.far_in[way].astype(F32)).astype(BF16)
                self.near(way, way).start()

        def finish(self):
            self.own(3)
            self.copy(self.near_in, self.near_in, 6, tp_of(1, False)).wait_recv()
            return self.acc[3] + self.near_in[0].astype(F32) + self.near_in[1].astype(F32)

        def drain(self):
            remote(self.bytes_ref, self.bytes_ref, rs_send.at[self.n], rs_recv.at[self.n, 0], fs,
                   tp_of(1, False)).wait_send()

    width = tokens_ref.shape[1]

    def normalize():
        total = None
        for t in range(N_TP):
            v = tok1[t].astype(F32)
            s = jnp.sum(v * v, axis=1, keepdims=True)
            total = s if total is None else total + s
        r = lax.rsqrt(total / (N_TP * width) + EPSILON)
        for t in range(N_TP):
            cols = slice(t * width, (t + 1) * width)
            normed[:, cols] = (tok1[t].astype(F32) * r * mixer_gain_ref[:, cols]).astype(BF16)

    def plane_rows(ref, zz, cols, small=False):
        rows = []
        for j in range(RING):
            straight = 1 if small else 0
            first = jnp.where(core == straight, j, zz)
            second = jnp.where(core == straight, zz, j)
            d = (first - (q if small else p) + RING) % RING
            at = jnp.where((d >= 1) & (d <= HOPS), 2 * d - 1, (2 * (RING - d)) % (2 * RING))
            rows.append(ref[second, at, :, cols])
        return rows

    def all_rows(ref, cols):
        return jnp.concatenate([r for zz in range(RING) for r in plane_rows(ref, zz, cols, True)], axis=0)

    def set_of(*bufs, low=None):
        return bufs if low is None else tuple(b.at[pl.ds(low * (b.shape[0] // 2), b.shape[0] // 2)] for b in bufs)

    gather1, gather2 = Gather(tok1, 0), Gather(tok2, 1)
    bufs2 = (sib_out2, sib_in2, ring_out2, far_in2, near_in2, acc2)
    scatter1 = Scatter(0, (sib_out1, sib_in1, ring_out1, far_in1, near_in1, acc1), tok1.at[0:7])
    scatter2 = Scatter(1, set_of(*bufs2, low=0), sib_out2.at[0:7])
    scatter3 = Scatter(2, set_of(*bufs2, low=1), sib_out2.at[0:7])

    value = {}

    def square_copy(d):
        ref = squares.at[tp]
        return remote(ref, ref, sq_send.at[0], sq_recv.at[0], fs, (tp + d) % N_TP)

    def spatial_branch():
        linear = jnp.dot(normed[...], all_rows(wp, slice(0, 128)), preferred_element_type=F32)
        spatial = jax.nn.gelu(linear * spatial_scale_ref[...])
        sq = spatial * spatial
        sq_high = sq.astype(BF16)
        sq_low = (sq - sq_high.astype(F32)).astype(BF16)
        ones = jnp.ones((8, 128), BF16)
        squares[tp] = nt_dot(ones, sq_high) + nt_dot(ones, sq_low)
        for d in range(1, N_TP):
            square_copy(d).start()
        value["gained"] = (spatial * spatial_gain_ref[...]).astype(BF16)

    def content_branch():
        linear = jnp.dot(normed[...], all_rows(wc, slice(0, 128)), preferred_element_type=F32)
        value["content"] = jax.nn.gelu(linear * content_scale_ref[...])
        causal = (
            lax.broadcasted_iota(jnp.int32, (BLOCK, BLOCK), 1)
            <= lax.broadcasted_iota(jnp.int32, (BLOCK, BLOCK), 0)
        )
        value["mixing"] = jnp.where(causal, mixing_ref[0].astype(F32), 0.0)
        value["bias"] = jnp.transpose(jnp.broadcast_to(bias_ref[...], (BLOCK, BLOCK)))

    def square_wait():
        ref = squares.at[0:N_TP - 1]
        remote(ref, ref, sq_send.at[0], sq_recv.at[0], fs, tp_of(1, False)).wait_recv()

    def mix():
        total_sq = squares[0]
        for t in range(1, N_TP):
            total_sq = total_sq + squares[t]
        row_scale = lax.rsqrt(total_sq[0:1] / (N_TP * 128) + EPSILON)
        gated = []
        for b in range(tokens_ref.shape[0] // BLOCK):
            rows = slice(b * BLOCK, (b + 1) * BLOCK)
            mixing_b = (value["mixing"] * row_scale[:, rows]).astype(BF16)
            mixed = jnp.dot(mixing_b, value["gained"][rows], preferred_element_type=F32) + value["bias"]
            gated.append((value["content"][rows] * mixed).astype(BF16))
        value["gated"] = jnp.concatenate(gated, axis=0)

    def project_blocks(k, dx):
        return tuple(
            nt_dot(value["gated"], jnp.concatenate(plane_rows(wc, tp_of(dx, other), slice(128, 256), True), axis=0))
            for other in (True, False))

    def middle():
        value["middle"] = (tokens_ref[...].astype(F32) + scatter1.finish()).astype(BF16)
        tok2[tp] = value["middle"]
        gather2.begin()

    def up_part(dxs, first=False):
        blocks = [tp_of(dx, other) for dx in dxs for other in (False, True)]
        terms = []
        for t in blocks:
            v = tok2[t].astype(F32)
            s = jnp.sum(v * v, axis=1, keepdims=True)
            value["sum"] = s if first and not terms else value["sum"] + s
            gain = channel_gain_ref[:, pl.ds(pl.multiple_of(t * width, 128), width)]
            terms.append((v * gain).astype(BF16))
        left = jnp.concatenate(terms, axis=1)
        for k in range(2):
            for low in range(0, 512, 256):
                cols = slice(low, low + 256)
                right = jnp.concatenate([r for t in blocks for r in plane_rows(wu.at[k], t, cols)], axis=0)
                at = slice(k * 512 + low, k * 512 + low + 256)
                part = jnp.dot(left, right, preferred_element_type=F32)
                up_acc[:, at] = part if first else up_acc[:, at] + part

    def activate():
        r = lax.rsqrt(value["sum"] / (N_TP * width) + EPSILON)
        up = jnp.maximum(up_acc[...] * r * up_scale_ref[...], 0.0)
        hidden[...] = (up * up).astype(BF16)

    def split_middle():
        natural = lax.broadcasted_iota(jnp.int32, (width, width), 0)
        split = lax.broadcasted_iota(jnp.int32, (width, width), 1)
        value["order"] = (
            natural == ((split % 128) // 16) * 32 + (split // 128) * 16 + split % 16
        ).astype(F32).astype(BF16)
        value["split"] = jnp.dot(value["middle"], value["order"], preferred_element_type=F32)

    def down_half(ref):
        def blocks_of(k, dx):
            rows = [
                jnp.concatenate(halves, axis=1)
                for other in (True, False)
                for halves in zip(*(plane_rows(ref.at[i], tp_of(dx, other), slice(0, 512)) for i in range(2)))
            ]
            both = nt_dot(hidden[...], jnp.concatenate(rows, axis=0))
            return both[:, 0:128], both[:, 128:256]

        return blocks_of

    def half_out(scatter, cols):
        rounded = (value["split"][:, cols] + scatter.finish()).astype(BF16)
        return nt_dot(rounded, value["order"][:, cols])

    def first_out():
        value["out"] = half_out(scatter2, slice(0, 128))

    def second_out():
        out_ref[...] = (value["out"] + half_out(scatter3, slice(128, 256))).astype(BF16)

    def late_fetches():
        for i in (1, 4, 5, 6, 7, 8, 11, 13):
            fetches[i].wait()

    small_send(SP)
    first_send(U, 0)
    small_send(SC)
    second_send(Uo)
    gather1.begin()
    second_send(D1o)
    first_send(D0, 0)
    second_send(D0o)
    first_send(D1, 0)
    first_forward(U, 1)
    small_wait(SP, 0)
    second_send(Ua)
    second_send(SPa)
    first_forward(D0, 1)
    small_wait(SC, 0)
    second_send(SCa)
    small_wait(SP, 1)
    second_send(SPb)
    first_forward(D1, 1)
    forward(D1o, 1)
    small_wait(SC, 1)
    second_send(SCb)
    first_forward(U, 2)
    forward(SPa, 1)
    second_send(D0a)
    gather1.pass_on()
    forward(Uo, 1)
    forward(SPb, 1)
    first_forward(D1, 2)
    forward(SCa, 1)
    forward(D0o, 1)
    first_forward(D0, 2)
    forward(SCb, 1)
    second_send(D1a)
    forward(SPa, 2)
    first_forward(U, 3)
    forward(SPb, 2)
    forward(D1o, 2)
    forward(SCa, 2)
    first_forward(D0, 3)
    first_forward(D1, 3)
    gather1.near()
    forward(Ua, 1)
    forward(D1a, 1)
    forward(SCb, 2)
    first_wait(U)
    gather1.far()
    forward(SPa, 3)
    gather1.wait(0, 1, 2, 3)
    second_send(Ub)
    forward(SPb, 3)
    late_fetches()
    normalize()
    first_wait(D1)
    forward(SCa, 3)
    forward(D0o, 2)
    second_send(D1b)
    forward(SCb, 3)
    forward(D1o, 3)
    first_wait(D0)
    second_wait(SPb)
    forward(Uo, 2)
    forward(Ua, 2)
    second_wait(SPa)
    spatial_branch()
    forward(D0a, 1)
    second_wait(SCb)
    forward(Ub, 1)
    second_wait(SCa)
    content_branch()
    second_send(D0b)
    square_wait()
    forward(D1a, 2)
    mix()
    scatter1.begin(project_blocks)
    forward(D1b, 1)
    forward(Uo, 3)
    scatter1.combine()
    forward(Ub, 2)
    forward(D0b, 1)
    forward(Ua, 3)
    middle()
    forward(D1b, 2)
    forward(Ub, 3)
    second_wait(Uo)
    forward(D0a, 2)
    gather2.pass_on()
    gather2.wait(0)
    forward(D0b, 2)
    forward(D0o, 3)
    split_middle()
    forward(D1a, 3)
    gather2.near()
    forward(D1b, 3)
    second_wait(Ub)
    gather2.wait(1, 2)
    second_wait(Ua)
    up_part((0,), True)
    forward(D0a, 3)
    gather2.far()
    up_part((-1, 1))
    gather2.wait(3)
    forward(D0b, 3)
    up_part((2,))
    second_wait(D0o)
    activate()
    second_wait(D1b)
    second_wait(D1a)
    second_wait(D1o)
    scatter3.begin(down_half(wd1))
    second_wait(D0a)
    second_wait(D0b)
    scatter2.begin(down_half(wd0))
    scatter3.combine()
    scatter2.combine()
    first_out()
    second_out()
    for u in range(5):
        ref = units[u].at[0, 0:7] if u <= SC else units[u].at[:, 0, 0:7]
        remote(ref, ref, w1_send.at[u], w1_recv.at[u, 0], fs, tp_of(1, False)).wait_send()
    for g in range(13):
        ref = group(g, pl.ds(0, 7))
        remote(ref, ref, w2_send.at[g], w2_recv.at[g, 0], fs, tp_of(1, False)).wait_send()
    gather1.drain()
    gather2.drain()
    scatter1.drain()
    scatter2.drain()
    scatter3.drain()
    remote(squares.at[0:7], squares.at[0:7], sq_send.at[0], sq_recv.at[0], fs, tp_of(1, False)).wait_send()


def shards(
    tokens, mixer_gain, w_content, w_spatial, content_scale, spatial_scale, spatial_gain, block_mixing,
    block_bias, w_project, project_scale, channel_gain, w_up, up_scale, w_down, down_scale,
):
    rows, width = tokens.shape
    row = lambda v: v.reshape(1, -1)
    inputs = (
        tokens, row(mixer_gain), w_content, w_spatial, row(content_scale), row(spatial_scale),
        row(spatial_gain), block_mixing, block_bias, w_project.T, row(project_scale), row(channel_gain),
        w_up, row(up_scale), w_down.T, row(down_scale),
    )
    vmem = pltpu.VMEM
    dma = pltpu.SemaphoreType.DMA
    anywhere = pl.BlockSpec(memory_space=pl.ANY)
    return pl.pallas_call(
        layer_kernel,
        out_shape=pltpu.VMEM((rows, width), BF16),
        in_specs=[anywhere] * N_INPUTS,
        out_specs=pl.BlockSpec(memory_space=pltpu.VMEM),
        scratch_shapes=[vmem(v.shape, v.dtype) for v in inputs] + [
            vmem((RING, RING, SLICE, 128), BF16),
            vmem((RING, RING, SLICE, 256), BF16),
            vmem((2, RING, RING, SLICE, 512), BF16),
            vmem((2, RING, RING, SLICE // 2, 512), BF16),
            vmem((2, RING, RING, SLICE // 2, 512), BF16),
            vmem((N_TP, rows, width), BF16),
            vmem((N_TP, rows, width), BF16),
            vmem((rows, N_TP * width), BF16),
            vmem((N_TP, 8, rows), F32),
            vmem((rows, w_up.shape[1]), BF16),
            vmem((rows, w_up.shape[1]), F32),
            vmem((4, rows, 256), BF16), vmem((4, rows, 256), BF16), vmem((3, rows, 256), BF16),
            vmem((2, rows // 2, 256), BF16), vmem((2, rows, 256), BF16), vmem((4, rows, 256), F32),
            vmem((8, rows, 128), BF16), vmem((8, rows, 128), BF16), vmem((6, rows, 128), BF16),
            vmem((4, rows // 2, 128), BF16), vmem((4, rows, 128), BF16), vmem((8, rows, 128), F32),
            dma((N_INPUTS,)), dma((5,)), dma((5, HOPS)), dma((13,)), dma((13, HOPS)),
            dma((2,)), dma((2, 10)), dma((3,)), dma((3, 7)), dma((1,)), dma((1,)),
        ],
        compiler_params=pltpu.CompilerParams(
            collective_id=0, has_side_effects=True, vmem_limit_bytes=56 * 1024 * 1024),
        name="layer",
    )(*inputs)


def solution(mesh):
    return jax.shard_map(
        shards,
        mesh=mesh,
        in_specs=(
            P("fs", "tp"), P(), P("fs", "tp"), P("fs", "tp"), P("tp"), P("tp"), P("tp"),
            P("tp", None, None), P("tp", None), P("tp", "fs"), P("fs"), P(), P("fs", "tp"), P("tp"),
            P("tp", "fs"), P("fs"),
        ),
        out_specs=P("fs", "tp"),
        check_vma=False,
    )
```

```python
import jax
import jax.numpy as jnp
from jax import lax
from jax.experimental import pallas as pl
from jax.experimental.pallas import tpu as pltpu
from jax.sharding import PartitionSpec as P

EPSILON = 1e-06
MESH = pl.DeviceIdType.MESH
F32 = jnp.float32
BF16 = jnp.bfloat16

RING = 8
HOPS = RING // 2
CHIPS_X = 4
N_TP = 2 * CHIPS_X
SLICE = 32
BLOCK = 128
N_INPUTS = 16


def nt_dot(left, right):
    return lax.dot_general(left, right, (((1,), (1,)), ((), ())), preferred_element_type=F32)


def layer_kernel(*refs):
    hbm = refs[:N_INPUTS]
    out_ref = refs[N_INPUTS]
    inputs = refs[N_INPUTS + 1:2 * N_INPUTS + 1]
    (
        tokens_ref, mixer_gain_ref, w_content_ref, w_spatial_ref, content_scale_ref, spatial_scale_ref,
        spatial_gain_ref, mixing_ref, bias_ref, w_project_ref, project_scale_ref, channel_gain_ref,
        w_up_ref, up_scale_ref, w_down_ref, down_scale_ref,
    ) = inputs
    (
        wp, wc, wu, wd0, wd1, tok1, tok2, normed, squares, hidden, up_acc,
        sib_out1, sib_in1, ring_out1, far_in1, near_in1, acc1,
        sib_out2, sib_in2, ring_out2, far_in2, near_in2, acc2,
        in_sem, w1_send, w1_recv, w2_send, w2_recv,
        ag_send, ag_recv, rs_send, rs_recv, sq_send, sq_recv,
    ) = refs[2 * N_INPUTS + 1:]
    fs, tp = lax.axis_index("fs"), lax.axis_index("tp")
    z, y = fs // RING, fs % RING
    x, core = tp // 2, tp % 2
    p = jnp.where(core == 0, y, z)
    q = jnp.where(core == 0, z, y)

    def fs_of(pp, qq):
        return jnp.where(core == 0, qq * RING + pp, pp * RING + qq)

    def tp_of(dx, other):
        c = (1 - core) if other else core
        return 2 * ((x + dx + CHIPS_X) % CHIPS_X) + c

    first_next = (fs_of((p + 1) % RING, q), fs_of((p + RING - 1) % RING, q))
    second_next = (fs_of(p, (q + 1) % RING), fs_of(p, (q + RING - 1) % RING))

    barrier = pltpu.get_barrier_semaphore()
    for to in tuple(fs_of(p, (q + d) % RING) for d in range(1, RING)) + first_next:
        pl.semaphore_signal(barrier, inc=1, device_id=(to, tp), device_id_type=MESH)
    for d in range(1, N_TP):
        pl.semaphore_signal(barrier, inc=1, device_id=(fs, (tp + d) % N_TP), device_id_type=MESH)
    fetches = [pltpu.make_async_copy(hbm[i], inputs[i], in_sem.at[i]) for i in range(N_INPUTS)]
    for i in (2, 3, 9, 10, 0, 12, 14, 15, 1, 4, 5, 6, 7, 8, 11, 13):
        fetches[i].start()

    def remote(src, dst, ss, rs, to_fs, to_tp):
        return pltpu.make_async_remote_copy(
            src_ref=src, dst_ref=dst, send_sem=ss, recv_sem=rs,
            device_id=(to_fs, to_tp), device_id_type=MESH,
        )

    eye = (
        lax.broadcasted_iota(jnp.int32, (SLICE, SLICE), 0)
        == lax.broadcasted_iota(jnp.int32, (SLICE, SLICE), 1)
    )

    def scaled(w, scale):
        column = jnp.sum(jnp.where(eye, scale, 0.0), axis=1, keepdims=True)
        return (w.astype(BF16).astype(F32) * column).astype(BF16)

    for i in (2, 3, 9, 10):
        fetches[i].wait()
    wp[p, 0] = w_spatial_ref[...].astype(BF16)
    wc[p, 0, :, 0:128] = w_content_ref[...].astype(BF16)
    wc[p, 0, :, 128:256] = scaled(w_project_ref[...], project_scale_ref[...])
    for i in (0, 12, 14, 15):
        fetches[i].wait()
    tok1[tp] = tokens_ref[...]
    down = scaled(w_down_ref[...], down_scale_ref[...])
    for k in range(2):
        cols = slice(k * 512, (k + 1) * 512)
        wu[k, q, 0] = w_up_ref[:, cols].astype(BF16)
        wd0[k, q, 0] = down[0:16, cols]
        wd1[k, q, 0] = down[16:32, cols]
    pl.semaphore_wait(barrier, RING - 1 + 2 + N_TP - 1)

    SP, SC, U, D0, D1 = range(5)
    units = (wp, wc, wu, wd0, wd1)

    def first_copy(u, src, dst, to, sem, part=None):
        if u <= SC:
            src_ref, dst_ref = units[u].at[p, src], units[u].at[p, dst]
        else:
            lead = slice(None) if part is None else part
            src_ref, dst_ref = units[u].at[lead, q, src], units[u].at[lead, q, dst]
        return remote(src_ref, dst_ref, w1_send.at[u], w1_recv.at[u, sem], to, tp)

    places = {0: 0, 1: 1, -1: 2, 2: 3, -2: 4, 3: 5, -3: 6, 4: 7, -4: 7}

    def first_send(u, step):
        for way in range(2):
            sign = 1 if way else -1
            first_copy(u, places[sign * step], places[sign * (step + 1)], first_next[way], step,
                       way if step == HOPS - 1 else None).start()

    def small_send(u):
        for d in (1, -1, 2, -2, 3, -3, 4):
            first_copy(u, 0, places[-d], fs_of(p, (q + d + RING) % RING), 0 if abs(d) == 1 else 1).start()

    def small_wait(u, sem):
        ref = units[u].at[0, 0:2] if sem == 0 else units[u].at[0, 0:5]
        remote(ref, ref, w1_send.at[u], w1_recv.at[u, sem], first_next[0], tp).wait_recv()

    def first_wait(u, distance=HOPS):
        n = 1 if distance == HOPS else 2
        ref = units[u].at[:, 0, 0:n]
        remote(ref, ref, w1_send.at[u], w1_recv.at[u, distance - 1], first_next[0], tp).wait_recv()

    def first_forward(u, step):
        first_wait(u, step)
        first_send(u, step)

    SPa, SPb, SCa, SCb, Uo, Ua, Ub, D0o, D0a, D0b, D1o, D1a, D1b = range(13)
    SMALL = 4
    groups = [(u, low, n) for u in (SP, SC) for low, n in ((0, 3), (3, 5))]
    groups += [(u, low, n) for u in (U, D0, D1) for low, n in ((0, 1), (1, 2), (3, 5))]

    def group(g, at, lead=slice(None)):
        u, low, n = groups[g]
        shards_of = pl.ds(low, n)
        return units[u].at[at, shards_of] if g < SMALL else units[u].at[lead, at, shards_of]

    def second_copy(g, way, step):
        start, to = (p, first_next) if g < SMALL else (q, second_next)
        at = (start + (step if way else -step) + RING) % RING
        ref = group(g, at)
        if step == HOPS - 1:
            ref = ref.at[:, pl.ds(way * (SLICE // 2), SLICE // 2)] if g < SMALL else group(g, at, way)
        return remote(ref, ref, w2_send.at[g], w2_recv.at[g, step], to[way], tp)

    def second_send(g, step=0):
        for way in range(2):
            second_copy(g, way, step).start()

    def second_wait(g, step=HOPS - 1):
        ref = group(g, 0) if step == HOPS - 1 else group(g, pl.ds(0, 2))
        remote(ref, ref, w2_send.at[g], w2_recv.at[g, step], second_next[0], tp).wait_recv()

    def forward(g, step):
        second_wait(g, step - 1)
        second_send(g, step)

    half = tokens_ref.shape[0] // 2

    class Gather:
        def __init__(self, buf, n):
            self.buf, self.n = buf, n

        def copy(self, k, arriving=False):
            dx = (0, -1, 1, 2, 0, 0, 0, 0, -1, 1)[k]
            if arriving and k >= 4:
                dx = (-1, 1, -1, 1, -2, 2)[k - 4]
            ref = self.buf.at[tp_of(dx, arriving and k < 4)]
            if k >= 4:
                ref = ref.at[pl.ds((k % 2 if k // 2 != 3 else 1 - k % 2) * half, half)]
            to = tp_of(0, True) if k < 4 else tp_of((1, -1)[k % 2], False)
            return remote(ref, ref, ag_send.at[self.n], ag_recv.at[self.n, k], fs, to)

        def begin(self):
            for k in (4, 5, 6, 7, 0):
                self.copy(k).start()

        def pass_on(self):
            for k in range(2):
                self.copy(4 + k, True).wait_recv()
                self.copy(8 + k).start()

        def near(self):
            for k in range(2):
                self.copy(6 + k, True).wait_recv()
                self.copy(1 + k).start()

        def far(self):
            for k in range(2):
                self.copy(8 + k, True).wait_recv()
            self.copy(3).start()

        def wait(self, *which):
            for k in which:
                self.copy(k, True).wait_recv()

        def drain(self):
            ref = self.buf.at[0:7]
            remote(ref, ref, ag_send.at[self.n], ag_recv.at[self.n, 0], fs, tp_of(1, False)).wait_send()

    class Scatter:
        order = (2, 1, -1, 0)

        def __init__(self, n, bufs, bytes_ref):
            self.n, self.bytes_ref = n, bytes_ref
            self.sib_out, self.sib_in, self.ring_out, self.far_in, self.near_in, self.acc = bufs

        def copy(self, src, dst, k, to):
            return remote(src, dst, rs_send.at[self.n], rs_recv.at[self.n, k], fs, to)

        def across(self, k):
            return self.copy(self.sib_out.at[k], self.sib_in.at[k], k, tp_of(0, True))

        def far(self, way):
            return self.copy(self.ring_out.at[0, pl.ds(way * half, half)], self.far_in.at[way], 4 + way,
                             tp_of((1, -1)[way], False))

        def near(self, way, part):
            rows = pl.ds(part * half, half)
            return self.copy(self.ring_out.at[1 + way, rows], self.near_in.at[way, rows], 6,
                             tp_of((1, -1)[way], False))

        def begin(self, blocks_of):
            for k, dx in enumerate(self.order):
                across, own = blocks_of(k, dx)
                self.sib_out[k] = across.astype(BF16)
                self.across(k).start()
                self.acc[k] = own
                if k > 1:
                    self.own(k - 2)
            self.own(2)

        def own(self, k):
            self.across(k).wait_recv()
            value = self.acc[k] + self.sib_in[k].astype(F32)
            if k == 0:
                self.ring_out[0] = value.astype(BF16)
                self.far(0).start()
                self.far(1).start()
            else:
                self.acc[k] = value
                if k < 3:
                    part = 2 - k
                    rows = slice(part * half, (part + 1) * half)
                    self.ring_out[k, rows] = value[rows].astype(BF16)
                    self.near(k - 1, part).start()

        def combine(self):
            for way in range(2):
                self.far(way).wait_recv()
                rows = slice(way * half, (way + 1) * half)
                self.ring_out[1 + way, rows] = (
                    self.acc[1 + way, rows] + self.far_in[way].astype(F32)).astype(BF16)
                self.near(way, way).start()

        def finish(self):
            self.own(3)
            self.copy(self.near_in, self.near_in, 6, tp_of(1, False)).wait_recv()
            return self.acc[3] + self.near_in[0].astype(F32) + self.near_in[1].astype(F32)

        def drain(self):
            remote(self.bytes_ref, self.bytes_ref, rs_send.at[self.n], rs_recv.at[self.n, 0], fs,
                   tp_of(1, False)).wait_send()

    width = tokens_ref.shape[1]

    def normalize():
        total = None
        for t in range(N_TP):
            v = tok1[t].astype(F32)
            s = jnp.sum(v * v, axis=1, keepdims=True)
            total = s if total is None else total + s
        r = lax.rsqrt(total / (N_TP * width) + EPSILON)
        for t in range(N_TP):
            cols = slice(t * width, (t + 1) * width)
            normed[:, cols] = (tok1[t].astype(F32) * r * mixer_gain_ref[:, cols]).astype(BF16)

    def plane_rows(ref, zz, cols, small=False):
        rows = []
        for j in range(RING):
            straight = 1 if small else 0
            first = jnp.where(core == straight, j, zz)
            second = jnp.where(core == straight, zz, j)
            d = (first - (q if small else p) + RING) % RING
            at = jnp.where((d >= 1) & (d <= HOPS), 2 * d - 1, (2 * (RING - d)) % (2 * RING))
            rows.append(ref[second, at, :, cols])
        return rows

    def all_rows(ref, cols):
        return jnp.concatenate([r for zz in range(RING) for r in plane_rows(ref, zz, cols, True)], axis=0)

    def set_of(*bufs, low=None):
        return bufs if low is None else tuple(b.at[pl.ds(low * (b.shape[0] // 2), b.shape[0] // 2)] for b in bufs)

    gather1, gather2 = Gather(tok1, 0), Gather(tok2, 1)
    bufs2 = (sib_out2, sib_in2, ring_out2, far_in2, near_in2, acc2)
    scatter1 = Scatter(0, (sib_out1, sib_in1, ring_out1, far_in1, near_in1, acc1), tok1.at[0:7])
    scatter2 = Scatter(1, set_of(*bufs2, low=0), sib_out2.at[0:7])
    scatter3 = Scatter(2, set_of(*bufs2, low=1), sib_out2.at[0:7])

    value = {}

    def square_copy(d):
        ref = squares.at[tp]
        return remote(ref, ref, sq_send.at[0], sq_recv.at[0], fs, (tp + d) % N_TP)

    def spatial_branch():
        linear = jnp.dot(normed[...], all_rows(wp, slice(0, 128)), preferred_element_type=F32)
        spatial = jax.nn.gelu(linear * spatial_scale_ref[...])
        sq = spatial * spatial
        sq_high = sq.astype(BF16)
        sq_low = (sq - sq_high.astype(F32)).astype(BF16)
        ones = jnp.ones((8, 128), BF16)
        squares[tp] = nt_dot(ones, sq_high) + nt_dot(ones, sq_low)
        for d in range(1, N_TP):
            square_copy(d).start()
        value["gained"] = (spatial * spatial_gain_ref[...]).astype(BF16)

    def content_branch():
        linear = jnp.dot(normed[...], all_rows(wc, slice(0, 128)), preferred_element_type=F32)
        value["content"] = jax.nn.gelu(linear * content_scale_ref[...])
        causal = (
            lax.broadcasted_iota(jnp.int32, (BLOCK, BLOCK), 1)
            <= lax.broadcasted_iota(jnp.int32, (BLOCK, BLOCK), 0)
        )
        value["mixing"] = jnp.where(causal, mixing_ref[0].astype(F32), 0.0)
        value["bias"] = jnp.transpose(jnp.broadcast_to(bias_ref[...], (BLOCK, BLOCK)))

    def square_wait():
        ref = squares.at[0:N_TP - 1]
        remote(ref, ref, sq_send.at[0], sq_recv.at[0], fs, tp_of(1, False)).wait_recv()

    def mix():
        total_sq = squares[0]
        for t in range(1, N_TP):
            total_sq = total_sq + squares[t]
        row_scale = lax.rsqrt(total_sq[0:1] / (N_TP * 128) + EPSILON)
        gated = []
        for b in range(tokens_ref.shape[0] // BLOCK):
            rows = slice(b * BLOCK, (b + 1) * BLOCK)
            mixing_b = (value["mixing"] * row_scale[:, rows]).astype(BF16)
            mixed = jnp.dot(mixing_b, value["gained"][rows], preferred_element_type=F32) + value["bias"]
            gated.append((value["content"][rows] * mixed).astype(BF16))
        value["gated"] = jnp.concatenate(gated, axis=0)

    def project_blocks(k, dx):
        return tuple(
            nt_dot(value["gated"], jnp.concatenate(plane_rows(wc, tp_of(dx, other), slice(128, 256), True), axis=0))
            for other in (True, False))

    def middle():
        value["middle"] = (tokens_ref[...].astype(F32) + scatter1.finish()).astype(BF16)
        tok2[tp] = value["middle"]
        gather2.begin()

    def up_part(dxs, first=False, last=False):
        blocks = [tp_of(dx, other) for dx in dxs for other in (False, True)]
        terms = []
        for t in blocks:
            v = tok2[t].astype(F32)
            s = jnp.sum(v * v, axis=1, keepdims=True)
            value["sum"] = s if first and not terms else value["sum"] + s
            gain = channel_gain_ref[:, pl.ds(pl.multiple_of(t * width, 128), width)]
            terms.append((v * gain).astype(BF16))
        left = jnp.concatenate(terms, axis=1)
        if last:
            r = lax.rsqrt(value["sum"] / (N_TP * width) + EPSILON)
        for k in range(2):
            for low in range(0, 512, 256):
                cols = slice(low, low + 256)
                right = jnp.concatenate([r for t in blocks for r in plane_rows(wu.at[k], t, cols)], axis=0)
                at = slice(k * 512 + low, k * 512 + low + 256)
                part = jnp.dot(left, right, preferred_element_type=F32)
                if last:
                    up = jnp.maximum((up_acc[:, at] + part) * r * up_scale_ref[:, at], 0.0)
                    hidden[:, at] = (up * up).astype(BF16)
                else:
                    up_acc[:, at] = part if first else up_acc[:, at] + part

    def split_middle():
        natural = lax.broadcasted_iota(jnp.int32, (width, width), 0)
        split = lax.broadcasted_iota(jnp.int32, (width, width), 1)
        value["order"] = (
            natural == ((split % 128) // 16) * 32 + (split // 128) * 16 + split % 16
        ).astype(F32).astype(BF16)
        value["split"] = jnp.dot(value["middle"], value["order"], preferred_element_type=F32)

    def down_half(ref):
        def blocks_of(k, dx):
            rows = [
                jnp.concatenate(halves, axis=1)
                for other in (True, False)
                for halves in zip(*(plane_rows(ref.at[i], tp_of(dx, other), slice(0, 512)) for i in range(2)))
            ]
            both = nt_dot(hidden[...], jnp.concatenate(rows, axis=0))
            return both[:, 0:128], both[:, 128:256]

        return blocks_of

    def half_out(scatter, cols):
        rounded = (value["split"][:, cols] + scatter.finish()).astype(BF16)
        return nt_dot(rounded, value["order"][:, cols])

    def first_out():
        value["out"] = half_out(scatter2, slice(0, 128))

    def second_out():
        out_ref[...] = (value["out"] + half_out(scatter3, slice(128, 256))).astype(BF16)

    def late_fetches():
        for i in (1, 4, 5, 6, 7, 8, 11, 13):
            fetches[i].wait()

    small_send(SP)
    first_send(U, 0)
    small_send(SC)
    second_send(Uo)
    gather1.begin()
    second_send(D1o)
    first_send(D0, 0)
    second_send(D0o)
    first_send(D1, 0)
    first_forward(U, 1)
    small_wait(SP, 0)
    second_send(Ua)
    second_send(SPa)
    first_forward(D0, 1)
    small_wait(SC, 0)
    second_send(SCa)
    small_wait(SP, 1)
    second_send(SPb)
    first_forward(D1, 1)
    forward(D1o, 1)
    small_wait(SC, 1)
    second_send(SCb)
    first_forward(U, 2)
    forward(SPa, 1)
    second_send(D0a)
    gather1.pass_on()
    forward(Uo, 1)
    forward(SPb, 1)
    first_forward(D1, 2)
    forward(SCa, 1)
    forward(D0o, 1)
    first_forward(D0, 2)
    forward(SCb, 1)
    second_send(D1a)
    forward(SPa, 2)
    first_forward(U, 3)
    forward(SPb, 2)
    forward(D1o, 2)
    forward(SCa, 2)
    first_forward(D0, 3)
    first_forward(D1, 3)
    gather1.near()
    forward(Ua, 1)
    forward(D1a, 1)
    forward(SCb, 2)
    first_wait(U)
    gather1.far()
    forward(SPa, 3)
    gather1.wait(0, 1, 2, 3)
    second_send(Ub)
    forward(SPb, 3)
    late_fetches()
    normalize()
    first_wait(D1)
    forward(SCa, 3)
    forward(D0o, 2)
    second_send(D1b)
    forward(SCb, 3)
    forward(D1o, 3)
    first_wait(D0)
    second_wait(SPb)
    forward(Uo, 2)
    forward(Ua, 2)
    second_wait(SPa)
    spatial_branch()
    forward(D0a, 1)
    second_wait(SCb)
    forward(Ub, 1)
    second_wait(SCa)
    content_branch()
    second_send(D0b)
    square_wait()
    forward(D1a, 2)
    mix()
    scatter1.begin(project_blocks)
    forward(D1b, 1)
    forward(Uo, 3)
    scatter1.combine()
    forward(Ub, 2)
    forward(D0b, 1)
    forward(Ua, 3)
    middle()
    forward(D1b, 2)
    forward(Ub, 3)
    second_wait(Uo)
    forward(D0a, 2)
    gather2.pass_on()
    gather2.wait(0)
    forward(D0b, 2)
    forward(D0o, 3)
    split_middle()
    forward(D1a, 3)
    gather2.near()
    forward(D1b, 3)
    second_wait(Ub)
    gather2.wait(1, 2)
    second_wait(Ua)
    up_part((0,), True)
    forward(D0a, 3)
    gather2.far()
    up_part((-1, 1))
    gather2.wait(3)
    forward(D0b, 3)
    up_part((2,), last=True)
    second_wait(D0o)
    second_wait(D1b)
    second_wait(D1a)
    second_wait(D1o)
    scatter3.begin(down_half(wd1))
    second_wait(D0a)
    second_wait(D0b)
    scatter2.begin(down_half(wd0))
    scatter3.combine()
    scatter2.combine()
    first_out()
    second_out()
    for u in range(5):
        ref = units[u].at[0, 0:7] if u <= SC else units[u].at[:, 0, 0:7]
        remote(ref, ref, w1_send.at[u], w1_recv.at[u, 0], fs, tp_of(1, False)).wait_send()
    for g in range(13):
        ref = group(g, pl.ds(0, 7))
        remote(ref, ref, w2_send.at[g], w2_recv.at[g, 0], fs, tp_of(1, False)).wait_send()
    gather1.drain()
    gather2.drain()
    scatter1.drain()
    scatter2.drain()
    scatter3.drain()
    remote(squares.at[0:7], squares.at[0:7], sq_send.at[0], sq_recv.at[0], fs, tp_of(1, False)).wait_send()


def shards(
    tokens, mixer_gain, w_content, w_spatial, content_scale, spatial_scale, spatial_gain, block_mixing,
    block_bias, w_project, project_scale, channel_gain, w_up, up_scale, w_down, down_scale,
):
    rows, width = tokens.shape
    row = lambda v: v.reshape(1, -1)
    inputs = (
        tokens, row(mixer_gain), w_content, w_spatial, row(content_scale), row(spatial_scale),
        row(spatial_gain), block_mixing, block_bias, w_project.T, row(project_scale), row(channel_gain),
        w_up, row(up_scale), w_down.T, row(down_scale),
    )
    vmem = pltpu.VMEM
    dma = pltpu.SemaphoreType.DMA
    anywhere = pl.BlockSpec(memory_space=pl.ANY)
    return pl.pallas_call(
        layer_kernel,
        out_shape=pltpu.VMEM((rows, width), BF16),
        in_specs=[anywhere] * N_INPUTS,
        out_specs=pl.BlockSpec(memory_space=pltpu.VMEM),
        scratch_shapes=[vmem(v.shape, v.dtype) for v in inputs] + [
            vmem((RING, RING, SLICE, 128), BF16),
            vmem((RING, RING, SLICE, 256), BF16),
            vmem((2, RING, RING, SLICE, 512), BF16),
            vmem((2, RING, RING, SLICE // 2, 512), BF16),
            vmem((2, RING, RING, SLICE // 2, 512), BF16),
            vmem((N_TP, rows, width), BF16),
            vmem((N_TP, rows, width), BF16),
            vmem((rows, N_TP * width), BF16),
            vmem((N_TP, 8, rows), F32),
            vmem((rows, w_up.shape[1]), BF16),
            vmem((rows, w_up.shape[1]), F32),
            vmem((4, rows, 256), BF16), vmem((4, rows, 256), BF16), vmem((3, rows, 256), BF16),
            vmem((2, rows // 2, 256), BF16), vmem((2, rows, 256), BF16), vmem((4, rows, 256), F32),
            vmem((8, rows, 128), BF16), vmem((8, rows, 128), BF16), vmem((6, rows, 128), BF16),
            vmem((4, rows // 2, 128), BF16), vmem((4, rows, 128), BF16), vmem((8, rows, 128), F32),
            dma((N_INPUTS,)), dma((5,)), dma((5, HOPS)), dma((13,)), dma((13, HOPS)),
            dma((2,)), dma((2, 10)), dma((3,)), dma((3, 7)), dma((1,)), dma((1,)),
        ],
        compiler_params=pltpu.CompilerParams(
            collective_id=0, has_side_effects=True, vmem_limit_bytes=56 * 1024 * 1024),
        name="layer",
    )(*inputs)


def solution(mesh):
    return jax.shard_map(
        shards,
        mesh=mesh,
        in_specs=(
            P("fs", "tp"), P(), P("fs", "tp"), P("fs", "tp"), P("tp"), P("tp"), P("tp"),
            P("tp", None, None), P("tp", None), P("tp", "fs"), P("fs"), P(), P("fs", "tp"), P("tp"),
            P("tp", "fs"), P("fs"),
        ),
        out_specs=P("fs", "tp"),
        check_vma=False,
    )
```
